32 devices in a mesh: ep: 16 (over z, y, x), tp: 2 (over core).
Axes of the slice: x: 2, y: 2, z: 4, core: 2. Of those that a mesh axis runs over, the one named last changes fastest.
Arguments:
- tokens: bfloat16 [256, 2048], P('ep'), may hold values from -6 to 6
- state: float32 [256, 8, 128, 128], P('ep', 'tp'), may hold values from -6 to 6
- mix_gain: float32 [2048], replicated, may hold values from 0.1 to 1.9
- moe_gain: float32 [2048], replicated, may hold values from 0.1 to 1.9
- head_gain: float32 [128], replicated, may hold values from 0.1 to 1.9
- w_forget: bfloat16 [2048, 1024], P(None, 'tp'), may hold values from -0.125 to 0.125
- w_query: bfloat16 [2048, 1024], P(None, 'tp'), may hold values from -0.125 to 0.125
- w_input: bfloat16 [2048, 1024], P(None, 'tp'), may hold values from -0.125 to 0.125
- w_outgate: bfloat16 [2048, 1024], P(None, 'tp'), may hold values from -0.125 to 0.125
- lower_bound: float32 [1024], P('tp'), may hold values from 0 to 0.9
- w_mix_out: bfloat16 [1024, 2048], P('tp'), may hold values from -0.1875 to 0.1875
- routes: int32 [256, 6], P('ep'), may hold values from 0 to 15, all different within a row; in each aligned block of 16 rows (0 to 15, 16 to 31, ...) at most 16 rows name the same one
- route_scores: float32 [256, 6], P('ep'), may hold values from 0.05 to 1
- expert_gate: bfloat16 [16, 2048, 512], P('ep', None, 'tp'), may hold values from -0.125 to 0.125
- expert_up: bfloat16 [16, 2048, 512], P('ep', None, 'tp'), may hold values from -0.125 to 0.125
- expert_down: bfloat16 [16, 512, 2048], P('ep', 'tp'), may hold values from -0.25 to 0.25
- shared_gate: bfloat16 [2048, 512], P(None, 'tp'), may hold values from -0.125 to 0.125
- shared_up: bfloat16 [2048, 512], P(None, 'tp'), may hold values from -0.125 to 0.125
- shared_down: bfloat16 [512, 2048], P('tp'), may hold values from -0.25 to 0.25
Outputs:
- layer_out: bfloat16 [256, 2048], P('ep', 'tp')
- new_state: float32 [256, 8, 128, 128], P('ep', 'tp')
The draws below stay inside these ranges and needn't reach their ends.
Inputs may be any that keep to these rules, and one draw needn't show every extreme that they name: `routes`: each token names 6 different experts. Among the tokens of one index of ep no expert is named by more than 16 tokens, and in every draw some expert is named by exactly 16 tokens of some index of ep.
All inputs are finite; a program needn't handle non-finite values.
Results may differ from the reference program's by a relative error of at most 0.017.
Values may be sent and summed in bfloat16 or wider, within the bound.
No kernel may reach another device: no remote copies, remote signals or barrier semaphores. Data moves between devices by JAX's collectives and lax.ppermute only.
A program may use at most 128 MiB of HBM per device.

```python
import math
import jax
import jax.numpy as jnp
import numpy as np
from jax import lax

D = 2048
HEADS = 8
HEAD_KEY = 128
HEAD_VALUE = 128
FE = 512
TOP_K = 6
S_DEV = 16
EXPERTS = 16
SEQS = 256
CAP = 16
N_EP = 16


def steps_of(own_key, shape, pieces, smallest, largest):
    level = 1.0
    for position, parts in pieces:
        draws = jax.random.uniform(jax.random.fold_in(jax.random.fold_in(own_key, 6), position), (parts,), jnp.float32, smallest / len(pieces), largest / len(pieces))
        level = level * jnp.repeat(jnp.exp(draws), shape[position] // parts).reshape((-1,) + (1,) * (len(shape) - 1 - position))
    return level


def deal_out(own_key, own, number, rows, number_of, top, bound, slope):
    order = jax.random.permutation(own_key, number_of)
    heavy_load, usual = shares(number_of, rows * top, bound, slope, True), shares(number_of, rows * top, bound, slope, False)
    places = jnp.arange(number_of)

    def named(sizes, offset_by):
        used = int((sizes > 0).sum())
        fixed = max(1, used // 4)
        moved = fixed + (places - fixed + offset_by * (used - fixed)) % max(1, number_of - fixed)
        return jnp.zeros((number_of,), jnp.int32).at[order[jnp.where(places < fixed, places, moved)]].set(jnp.asarray(sizes, jnp.int32))

    sizes = jnp.where(number % 4 == 0, named(heavy_load, number // 4), named(usual, number - number // 4 - 1))
    mixed = jax.random.permutation(jax.random.fold_in(own, 3), number_of)
    giver, taker = mixed[0:number_of // 2 * 2:2], mixed[1:number_of // 2 * 2:2]
    margin = jnp.minimum(sizes[giver] - 1, bound - sizes[taker]) // 2
    margin = jnp.where((giver == order[0]) | (taker == order[0]) | (sizes[taker] == 0), 0, jnp.maximum(margin, 0))
    moved = jax.random.randint(jax.random.fold_in(own, 4), (number_of // 2,), 0, 1 << 20) % (margin + 1)
    sizes = sizes.at[giver].add(-moved).at[taker].add(moved)
    items = jnp.searchsorted(jnp.cumsum(sizes), jnp.arange(rows * top), side="right").astype(jnp.int32)
    grid = items.reshape(top, rows).T
    grid = grid[jax.random.permutation(jax.random.fold_in(own, 1), rows)]
    offset_by = jax.random.randint(jax.random.fold_in(own, 2), (rows, 1), 0, top)
    return jnp.take_along_axis(grid, (jnp.arange(top)[None, :] + offset_by) % top, axis=1)


def shares(number_of, total, most, slope, full):
    loads = [(1 << 20) // math.isqrt(standing ** slope) + 1 for standing in range(1, number_of + 1)]
    largest = most if full else min(most, max(-(-total // number_of), total * loads[0] // sum(loads)))
    least = 1 if total - largest >= number_of - 1 else 0
    counts, spare = [largest] + [least] * (number_of - 1), total - largest - least * (number_of - 1)
    while spare > 0:
        movable = [i for i in range(1, number_of) if counts[i] < largest] or [i for i in range(1, number_of) if counts[i] < most]
        mass, remaining = sum([loads[i] for i in movable]), spare
        for i in movable:
            extra = min(most - counts[i], max(1, remaining * loads[i] // mass), spare)
            counts[i] = counts[i] + extra
            spare = spare - extra
    return np.array(counts)


def centred(stream_key, shape, deviation, bound, shards=(), kind=jnp.bfloat16):
    array = jax.random.normal(stream_key, shape, jnp.float32) * deviation
    if len(shards) > 0:
        array = steps_of(stream_key, shape, shards, -0.22, 0.18) * array
    return jnp.clip(array, min=-bound, max=bound).astype(kind)


def setup_inputs(seed: int = 0) -> dict:
    keys = jax.random.split(jax.random.key(seed), 20)
    tokens = centred(keys[0], (SEQS, D), 1.0, 6.0, ((0, 16),))
    state = centred(keys[1], (SEQS, HEADS, HEAD_KEY, HEAD_VALUE), 1.0, 6.0, ((0, 16), (1, 2)), jnp.float32)
    mix_gain = jnp.clip(1.0 + 0.18 * jax.random.normal(keys[2], (D,), jnp.float32), 0.1, 1.9)
    moe_gain = jnp.clip(1.0 + 0.18 * jax.random.normal(keys[3], (D,), jnp.float32), 0.1, 1.9)
    head_gain = jnp.clip(1.0 + 0.18 * jax.random.normal(keys[4], (HEAD_VALUE,), jnp.float32), 0.1, 1.9)
    w_forget = centred(keys[5], (D, HEADS * HEAD_KEY), D ** -0.5, 0.125, ((1, 2),))
    w_query = centred(keys[6], (D, HEADS * HEAD_KEY), D ** -0.5, 0.125, ((1, 2),))
    w_input = centred(keys[7], (D, HEADS * HEAD_VALUE), D ** -0.5, 0.125, ((1, 2),))
    w_outgate = centred(keys[8], (D, HEADS * HEAD_VALUE), D ** -0.5, 0.125, ((1, 2),))
    lower_bound = jnp.clip(0.9 * jax.random.uniform(keys[9], (HEADS * HEAD_KEY,), jnp.float32) ** steps_of(keys[9], (HEADS * HEAD_KEY,), ((0, 2),), -0.2, 0.2), 0.0, 0.9)
    w_mix_out = centred(keys[10], (HEADS * HEAD_VALUE, D), (HEADS * HEAD_VALUE) ** -0.5, 0.1875, ((0, 2),))
    routes_keys = jax.random.split(jax.random.fold_in(keys[11], 1), SEQS // S_DEV)
    routes_turns = jax.random.permutation(jax.random.fold_in(keys[11], 3), SEQS // S_DEV)
    routes = jax.vmap(lambda own, number: deal_out(jax.random.fold_in(keys[11], 2), own, number, S_DEV, EXPERTS, TOP_K, CAP, 2))(routes_keys, routes_turns).reshape((SEQS, TOP_K))
    route_scores = jnp.clip(0.05 + 0.95 * jax.random.uniform(keys[12], (SEQS, TOP_K), jnp.float32) ** steps_of(keys[12], (SEQS, TOP_K), ((0, 16),), -0.2, 0.2), 0.05, 1.0)
    expert_gate = centred(keys[13], (EXPERTS, D, FE), D ** -0.5, 0.125, ((0, 16), (2, 2)))
    expert_up = centred(keys[14], (EXPERTS, D, FE), D ** -0.5, 0.125, ((0, 16), (2, 2)))
    expert_down = centred(keys[15], (EXPERTS, FE, D), FE ** -0.5, 0.25, ((0, 16), (1, 2)))
    shared_gate = centred(keys[16], (D, FE), D ** -0.5, 0.125, ((1, 2),))
    shared_up = centred(keys[17], (D, FE), D ** -0.5, 0.125, ((1, 2),))
    shared_down = centred(keys[18], (FE, D), FE ** -0.5, 0.25, ((0, 2),))
    return dict(tokens=tokens, state=state, mix_gain=mix_gain, moe_gain=moe_gain, head_gain=head_gain, w_forget=w_forget, w_query=w_query, w_input=w_input, w_outgate=w_outgate, lower_bound=lower_bound, w_mix_out=w_mix_out, routes=routes, route_scores=route_scores, expert_gate=expert_gate, expert_up=expert_up, expert_down=expert_down, shared_gate=shared_gate, shared_up=shared_up, shared_down=shared_down)


epsilon = 1e-06
routed_scale = 2.5

def rms_scale(values, gain):
    return values * lax.rsqrt(lax.optimization_barrier(jnp.mean(values * values, axis=-1, keepdims=True)) + epsilon) * gain

def rounded(values):
    return lax.optimization_barrier(values.astype(jnp.bfloat16)).astype(jnp.float32)

def halves_sum(operand, weight, split_at):
    first = jnp.dot(operand[:, :split_at], weight[:split_at], preferred_element_type=jnp.float32)
    second = jnp.dot(operand[:, split_at:], weight[split_at:], preferred_element_type=jnp.float32)
    return (rounded(first) + rounded(second)).astype(jnp.bfloat16)

def reference(tokens, state, mix_gain, moe_gain, head_gain, w_forget, w_query, w_input, w_outgate, lower_bound, w_mix_out, routes, route_scores, expert_gate, expert_up, expert_down, shared_gate, shared_up, shared_down):
    seq_count = tokens.shape[0]
    tokens_wide = tokens.astype(jnp.float32)
    normed = rms_scale(tokens_wide, mix_gain).astype(jnp.bfloat16)
    forget_pre = jnp.dot(normed, w_forget, preferred_element_type=jnp.float32).reshape(seq_count, HEADS, HEAD_KEY)
    query = jax.nn.silu(jnp.dot(normed, w_query, preferred_element_type=jnp.float32)).reshape(seq_count, HEADS, HEAD_KEY)
    input_val = jnp.dot(normed, w_input, preferred_element_type=jnp.float32).reshape(seq_count, HEADS, HEAD_VALUE)
    gate_pre = jnp.dot(normed, w_outgate, preferred_element_type=jnp.float32).reshape(seq_count, HEADS, HEAD_VALUE)
    bound_rows = lower_bound.reshape(HEADS, HEAD_KEY)
    forget = bound_rows + (1.0 - bound_rows) * jax.nn.sigmoid(forget_pre)
    key_gate = (1.0 - bound_rows) * jax.nn.sigmoid(-forget_pre)
    new_state = forget[..., None] * state + key_gate[..., None] * input_val[:, :, None, :]
    readout = jnp.einsum('shkv,shk->shv', new_state, query, precision=lax.Precision.HIGHEST)
    gated_out = (rms_scale(readout, head_gain) * jax.nn.silu(gate_pre)).astype(jnp.bfloat16)
    gated_out = gated_out.reshape(seq_count, HEADS * HEAD_VALUE)
    mixer_out = halves_sum(gated_out, w_mix_out, HEADS * HEAD_VALUE // 2)
    residual = tokens_wide + mixer_out.astype(jnp.float32)
    moe_rows = rms_scale(residual, moe_gain).astype(jnp.bfloat16)
    weights = route_scores / lax.optimization_barrier(jnp.sum(route_scores, axis=-1, keepdims=True)) * routed_scale
    shared_hidden = (jax.nn.silu(jnp.dot(moe_rows, shared_gate, preferred_element_type=jnp.float32)) * jnp.dot(moe_rows, shared_up, preferred_element_type=jnp.float32)).astype(jnp.bfloat16)
    shared_out = halves_sum(shared_hidden, shared_down, FE // 2)
    flat_routes = routes.reshape(-1)
    slot_count = N_EP * CAP
    rows_repeated = jnp.repeat(moe_rows, TOP_K, axis=0)

    def one_expert(totals, inputs):
        gate_w, up_w, down_w, expert_id = inputs
        chosen = flat_routes == expert_id
        slot_rank = (jnp.cumsum(chosen.astype(jnp.int32)) - 1).astype(jnp.int32)
        target = jnp.where(chosen, slot_rank, slot_count).astype(jnp.int32)
        buffer = jnp.zeros((slot_count, D), jnp.bfloat16).at[target].set(rows_repeated, mode='drop')
        hidden = (jax.nn.silu(jnp.dot(buffer, gate_w, preferred_element_type=jnp.float32)) * jnp.dot(buffer, up_w, preferred_element_type=jnp.float32)).astype(jnp.bfloat16)
        result = halves_sum(hidden, down_w, FE // 2)
        picked = result[jnp.clip(slot_rank, 0, slot_count - 1)].astype(jnp.float32)
        return (totals + jnp.where(chosen[:, None], picked, jnp.float32(0.0)), None)
    totals, _ = lax.scan(one_expert, jnp.zeros((seq_count * TOP_K, D), jnp.float32), (expert_gate, expert_up, expert_down, jnp.arange(EXPERTS, dtype=jnp.int32)))
    routed = lax.optimization_barrier(jnp.sum(totals.reshape(seq_count, TOP_K, D) * weights[:, :, None], axis=1))
    layer_out = (residual + routed + shared_out.astype(jnp.float32)).astype(jnp.bfloat16)
    return (layer_out, new_state)
```

```python
import jax
import jax.numpy as jnp
from jax import lax
from jax.sharding import PartitionSpec as P

epsilon = 1e-06
routed_scale = 2.5


def rms_scale(values, gain):
    return values * lax.rsqrt(jnp.mean(values * values, axis=-1, keepdims=True) + epsilon) * gain


def dot(a, b):
    return jnp.dot(a, b, preferred_element_type=jnp.float32)


def swap(values):
    return lax.ppermute(values, "tp", [(0, 1), (1, 0)])


def local(
    tokens,
    state,
    mix_gain,
    moe_gain,
    head_gain,
    w_forget,
    w_query,
    w_input,
    w_outgate,
    lower_bound,
    w_mix_out,
    routes,
    route_scores,
    expert_gate,
    expert_up,
    expert_down,
    shared_gate,
    shared_up,
    shared_down,
):
    seqs_here, full_width = tokens.shape
    heads_here = state.shape[1]
    key_width = state.shape[2]
    value_width = state.shape[3]
    n_ep = lax.axis_size("ep")
    n_tp = lax.axis_size("tp")
    tp_index = lax.axis_index("tp")
    half_width = full_width // n_tp
    half_rows = seqs_here // n_tp

    other_gate = swap(expert_gate[0])
    other_up = swap(expert_up[0])
    other_down = swap(expert_down[0])

    tokens_wide = tokens.astype(jnp.float32)
    normed = rms_scale(tokens_wide, mix_gain).astype(jnp.bfloat16)
    forget_pre = dot(normed, w_forget).reshape(seqs_here, heads_here, key_width)
    query = jax.nn.silu(dot(normed, w_query)).reshape(seqs_here, heads_here, key_width)
    input_val = dot(normed, w_input).reshape(seqs_here, heads_here, value_width)
    gate_pre = dot(normed, w_outgate).reshape(seqs_here, heads_here, value_width)
    bound_rows = lower_bound.reshape(heads_here, key_width)
    forget = bound_rows + (1.0 - bound_rows) * jax.nn.sigmoid(forget_pre)
    key_gate = (1.0 - bound_rows) * jax.nn.sigmoid(-forget_pre)
    new_state = forget[..., None] * state + key_gate[..., None] * input_val[:, :, None, :]
    readout = jnp.einsum("shkv,shk->shv", new_state, query, precision=lax.Precision.HIGHEST)
    gated_out = (rms_scale(readout, head_gain) * jax.nn.silu(gate_pre)).astype(jnp.bfloat16)
    gated_out = gated_out.reshape(seqs_here, heads_here * value_width)
    mix_part = dot(gated_out, w_mix_out).astype(jnp.bfloat16)
    mixer_out = mix_part.astype(jnp.float32) + swap(mix_part).astype(jnp.float32)
    residual = tokens_wide + mixer_out.astype(jnp.bfloat16).astype(jnp.float32)
    moe_rows = rms_scale(residual, moe_gain).astype(jnp.bfloat16)

    own_rows = lax.dynamic_slice_in_dim(moe_rows, tp_index * half_rows, half_rows, 0)
    outgoing = jnp.broadcast_to(own_rows[None], (n_ep, half_rows, full_width))
    arrived = lax.all_to_all(outgoing, "ep", 0, 0).reshape(n_ep * half_rows, full_width)

    shared_hidden = (
        jax.nn.silu(dot(moe_rows, shared_gate)) * dot(moe_rows, shared_up)
    ).astype(jnp.bfloat16)
    shared_part = dot(shared_hidden, shared_down).astype(jnp.bfloat16)
    own_start = tp_index * half_width
    other_start = (1 - tp_index) * half_width
    shared_own = lax.dynamic_slice_in_dim(shared_part, own_start, half_width, 1)
    shared_sent = lax.dynamic_slice_in_dim(shared_part, other_start, half_width, 1)
    shared_out = shared_own.astype(jnp.float32) + swap(shared_sent).astype(jnp.float32)

    def hidden_of(gate, up):
        return (jax.nn.silu(dot(arrived, gate)) * dot(arrived, up)).astype(jnp.bfloat16)

    expert_out = dot(hidden_of(expert_gate[0], expert_up[0]), expert_down[0]) + dot(
        hidden_of(other_gate, other_up), other_down
    )
    expert_out = expert_out.astype(jnp.bfloat16).reshape(n_ep, half_rows, n_tp, half_width)
    leaving = expert_out.transpose(0, 2, 1, 3).reshape(n_ep * n_tp, half_rows, half_width)
    returned = lax.all_to_all(leaving, ("ep", "tp"), 0, 0)
    returned = returned.reshape(n_ep, seqs_here, half_width).astype(jnp.float32)

    weights = route_scores / jnp.sum(route_scores, axis=-1, keepdims=True) * routed_scale
    chosen = routes[:, :, None] == jnp.arange(n_ep, dtype=jnp.int32)[None, None, :]
    expert_weight = jnp.sum(jnp.where(chosen, weights[:, :, None], 0.0), axis=1)
    routed = jnp.sum(returned * expert_weight.T[:, :, None], axis=0)
    residual_half = lax.dynamic_slice_in_dim(residual, own_start, half_width, 1)
    layer_out = (residual_half + routed + shared_out).astype(jnp.bfloat16)
    return (layer_out, new_state)


def solution(mesh):
    return jax.shard_map(
        local,
        mesh=mesh,
        in_specs=(
            P("ep", None),
            P("ep", "tp", None, None),
            P(),
            P(),
            P(),
            P(None, "tp"),
            P(None, "tp"),
            P(None, "tp"),
            P(None, "tp"),
            P("tp"),
            P("tp", None),
            P("ep", None),
            P("ep", None),
            P("ep", None, "tp"),
            P("ep", None, "tp"),
            P("ep", "tp", None),
            P(None, "tp"),
            P(None, "tp"),
            P("tp", None),
        ),
        out_specs=(P("ep", "tp"), P("ep", "tp", None, None)),
        check_vma=False,
    )
```

```python
import functools

import jax
import jax.numpy as jnp
from jax import lax
from jax.experimental import pallas as pl
from jax.experimental.pallas import tpu as pltpu
from jax.sharding import PartitionSpec as P

epsilon = 1e-06
routed_scale = 2.5
ANY = pl.BlockSpec(memory_space=pl.ANY)
VMEM = pl.BlockSpec(memory_space=pltpu.VMEM)


def rms_scale(values, gain):
    return values * lax.rsqrt(jnp.mean(values * values, axis=-1, keepdims=True) + epsilon) * gain


def dot(a, b):
    return jnp.dot(a, b, preferred_element_type=jnp.float32)


def silu(values):
    return values / (1.0 + jnp.exp(-values))


def sigmoid(values):
    return 1.0 / (1.0 + jnp.exp(-values))


def swap(values):
    return lax.ppermute(values, "tp", [(0, 1), (1, 0)])


def mixer_kernel(
    tokens_ref,
    mix_gain_ref,
    head_gain_ref,
    bound_ref,
    wf_hbm,
    wq_hbm,
    wi_hbm,
    wg_hbm,
    state_hbm,
    wm_hbm,
    part_ref,
    forget_ref,
    key_ref,
    input_ref,
    wf,
    wq,
    wi,
    wg,
    state,
    wm,
    readout_ref,
    sems,
):
    seqs, heads = state_hbm.shape[0], state_hbm.shape[1]
    width = state_hbm.shape[3]
    copies = {}

    def start(name, source, target):
        copies[name] = pltpu.make_async_copy(source, target, sems.at[len(copies)])
        copies[name].start()

    start("f", wf_hbm, wf)
    start("q", wq_hbm, wq)
    start("i", wi_hbm, wi)
    start("g", wg_hbm, wg)
    for h in range(heads):
        if h == heads - 1:
            start("m", wm_hbm, wm)
        start(h, state_hbm.at[:, h], state.at[h])

    tokens = tokens_ref[...].astype(jnp.float32)
    normed = rms_scale(tokens, mix_gain_ref[...]).astype(jnp.bfloat16)
    bound = bound_ref[...]
    copies["f"].wait()
    forget_pre = dot(normed, wf[...])
    forget = bound + (1.0 - bound) * sigmoid(forget_pre)
    key = (1.0 - bound) * sigmoid(-forget_pre)
    forget_ref[...] = forget
    key_ref[...] = key
    copies["q"].wait()
    query = silu(dot(normed, wq[...]))
    copies["i"].wait()
    input_val = dot(normed, wi[...])
    input_ref[...] = input_val
    copies["g"].wait()
    gate = silu(dot(normed, wg[...]))

    forget_query = forget * query
    key_query = key * query
    columns = [forget_query[:, h * width : (h + 1) * width] for h in range(heads)]
    rows_left = width - seqs * heads
    if rows_left:
        columns.append(jnp.zeros((rows_left, width), jnp.float32))
    turned = jnp.concatenate(columns, axis=0).T
    total = None
    pair = []
    for h in range(heads):
        copies[h].wait()
        for s in range(seqs):
            at = h * seqs + s
            readout_ref[s : s + 1, :] = jnp.sum(
                state[h, s] * turned[:, at : at + 1], axis=0, keepdims=True
            )
        here = slice(h * width, (h + 1) * width)
        fresh = jnp.sum(key_query[:, here], axis=-1, keepdims=True) * input_val[:, here]
        readout = readout_ref[...] + fresh
        pair.append((rms_scale(readout, head_gain_ref[...]) * gate[:, here]).astype(jnp.bfloat16))
        if h == heads - 1:
            copies["m"].wait()
    part_ref[...] = dot(jnp.concatenate(pair, axis=1), wm[...]).astype(jnp.bfloat16)


def mixer(tokens, mix_gain, head_gain, bound, wf, wq, wi, wg, state, wm):
    seqs, heads, width, _ = state.shape
    wide = jax.ShapeDtypeStruct((seqs, heads * width), jnp.float32)
    return pl.pallas_call(
        mixer_kernel,
        out_shape=(jax.ShapeDtypeStruct((seqs, wm.shape[1]), jnp.bfloat16), wide, wide, wide),
        in_specs=[VMEM] * 4 + [ANY] * 6,
        out_specs=(VMEM,) * 4,
        scratch_shapes=[pltpu.VMEM(w.shape, w.dtype) for w in (wf, wq, wi, wg)]
        + [
            pltpu.VMEM((heads, seqs, width, width), jnp.float32),
            pltpu.VMEM(wm.shape, wm.dtype),
            pltpu.VMEM((seqs, width), jnp.float32),
            pltpu.SemaphoreType.DMA((5 + heads,)),
        ],
        cost_estimate=pl.CostEstimate(
            flops=40_000_000_000, bytes_accessed=16 << 20, transcendentals=0
        ),
        name="mixer",
    )(tokens, mix_gain[None], head_gain[None], bound[None], wf, wq, wi, wg, state, wm)


def expert_kernel(x_ref, *refs):
    weights, out_ref = refs[:6], refs[6]
    x = x_ref[...]
    hidden = [
        (silu(dot(x, weights[3 * i][...])) * dot(x, weights[3 * i + 1][...])).astype(jnp.bfloat16)
        for i in range(2)
    ]
    senders, rows, width = out_ref.shape[0] // 2, out_ref.shape[1], out_ref.shape[2]
    for t in range(2):
        here = slice(t * width, (t + 1) * width)
        total = dot(hidden[0], weights[2][:, here]) + dot(hidden[1], weights[5][:, here])
        total = total.astype(jnp.bfloat16)
        for e in range(senders):
            out_ref[2 * e + t] = total[e * rows : (e + 1) * rows]


def expert(x, weights, out_shape):
    return pl.pallas_call(
        expert_kernel,
        out_shape=jax.ShapeDtypeStruct(out_shape, jnp.bfloat16),
        in_specs=[VMEM] * 7,
        out_specs=VMEM,
        compiler_params=pltpu.CompilerParams(vmem_limit_bytes=12 << 20),
        name="expert",
    )(x, *weights)


def local(
    tokens,
    state,
    mix_gain,
    moe_gain,
    head_gain,
    w_forget,
    w_query,
    w_input,
    w_outgate,
    lower_bound,
    w_mix_out,
    routes,
    route_scores,
    expert_gate,
    expert_up,
    expert_down,
    shared_gate,
    shared_up,
    shared_down,
):
    seqs_here, full_width = tokens.shape
    heads_here = state.shape[1]
    key_width = state.shape[2]
    n_ep = lax.axis_size("ep")
    n_tp = lax.axis_size("tp")
    tp_index = lax.axis_index("tp")
    half_width = full_width // n_tp
    half_rows = seqs_here // n_tp

    own = (expert_gate[0], expert_up[0], expert_down[0])
    other = tuple(swap(w) for w in own)

    mix_part, forget, key_gate, input_val = mixer(
        tokens,
        mix_gain,
        head_gain,
        lower_bound,
        w_forget,
        w_query,
        w_input,
        w_outgate,
        state,
        w_mix_out,
    )
    by_head = (seqs_here, heads_here, key_width)
    new_state = (
        forget.reshape(by_head)[..., None] * state
        + key_gate.reshape(by_head)[..., None] * input_val.reshape(by_head)[:, :, None, :]
    )
    mixer_out = mix_part.astype(jnp.float32) + swap(mix_part).astype(jnp.float32)
    residual = tokens.astype(jnp.float32) + mixer_out.astype(jnp.bfloat16).astype(jnp.float32)
    moe_rows = rms_scale(residual, moe_gain).astype(jnp.bfloat16)

    own_rows = lax.dynamic_slice_in_dim(moe_rows, tp_index * half_rows, half_rows, 0)
    outgoing = jnp.broadcast_to(own_rows[None], (n_ep, half_rows, full_width))
    arrived = lax.all_to_all(outgoing, "ep", 0, 0).reshape(n_ep * half_rows, full_width)

    shared_hidden = (
        jax.nn.silu(dot(moe_rows, shared_gate)) * dot(moe_rows, shared_up)
    ).astype(jnp.bfloat16)
    shared_part = dot(shared_hidden, shared_down).astype(jnp.bfloat16)
    own_start = tp_index * half_width
    other_start = (1 - tp_index) * half_width
    shared_own = lax.dynamic_slice_in_dim(shared_part, own_start, half_width, 1)
    shared_sent = lax.dynamic_slice_in_dim(shared_part, other_start, half_width, 1)
    shared_out = shared_own.astype(jnp.float32) + swap(shared_sent).astype(jnp.float32)

    leaving = expert(arrived, own + other, (n_ep * n_tp, half_rows, half_width))
    returned = lax.all_to_all(leaving, ("ep", "tp"), 0, 0)
    returned = returned.reshape(n_ep, seqs_here, half_width).astype(jnp.float32)

    weights = route_scores / jnp.sum(route_scores, axis=-1, keepdims=True) * routed_scale
    chosen = routes[:, :, None] == jnp.arange(n_ep, dtype=jnp.int32)[None, None, :]
    expert_weight = jnp.sum(jnp.where(chosen, weights[:, :, None], 0.0), axis=1)
    routed = jnp.sum(returned * expert_weight.T[:, :, None], axis=0)
    residual_half = lax.dynamic_slice_in_dim(residual, own_start, half_width, 1)
    layer_out = (residual_half + routed + shared_out).astype(jnp.bfloat16)
    return (layer_out, new_state)


def solution(mesh):
    return jax.shard_map(
        local,
        mesh=mesh,
        in_specs=(
            P("ep", None),
            P("ep", "tp", None, None),
            P(),
            P(),
            P(),
            P(None, "tp"),
            P(None, "tp"),
            P(None, "tp"),
            P(None, "tp"),
            P("tp"),
            P("tp", None),
            P("ep", None),
            P("ep", None),
            P("ep", None, "tp"),
            P("ep", None, "tp"),
            P("ep", "tp", None),
            P(None, "tp"),
            P(None, "tp"),
            P("tp", None),
        ),
        out_specs=(P("ep", "tp"), P("ep", "tp", None, None)),
        check_vma=False,
    )
```

```python
import jax
import jax.numpy as jnp
from jax import lax
from jax.experimental import pallas as pl
from jax.experimental.pallas import tpu as pltpu
from jax.sharding import PartitionSpec as P


epsilon = 1e-06
routed_scale = 2.5
HBM = pl.BlockSpec(memory_space=pltpu.HBM)
VMEM = pl.BlockSpec(memory_space=pltpu.VMEM)


def rms_scale(values, gain):
    return values * lax.rsqrt(jnp.mean(values * values, axis=-1, keepdims=True) + epsilon) * gain


def dot(a, b):
    return jnp.dot(a, b, preferred_element_type=jnp.float32)


def silu(values):
    return values / (1.0 + jnp.exp(-values))


def sigmoid(values):
    return 1.0 / (1.0 + jnp.exp(-values))


def swap(values):
    return lax.ppermute(values, "tp", [(0, 1), (1, 0)])


def in_hbm(*values):
    return tuple(pltpu.with_memory_space_constraint(v, pltpu.HBM) for v in values)


def mixer_kernel(*refs):
    sources, refs = refs[:10], refs[10:]
    part_ref, forget_ref, key_ref, input_ref = refs[:4]
    targets, readout_ref, sems = refs[4:14], refs[14], refs[15]
    tokens_ref, mix_gain, bound_ref, wf, wq, wi, wg, head_gain, state, wm = targets
    state_hbm = sources[8]
    heads, seqs, width, _ = state.shape
    copies = []

    def start(source, target):
        copies.append(pltpu.make_async_copy(source, target, sems.at[len(copies)]))
        copies[-1].start()

    for i in range(8):
        start(sources[i], targets[i])
    for h in range(heads):
        start(state_hbm.at[:, h], state.at[h])
        if h == heads - 2:
            start(sources[9], wm)
    of_tokens, of_gain, of_bound, of_wf, of_wq, of_wi, of_wg, of_head, *of_state = copies
    of_wm = of_state.pop(heads - 1)

    of_tokens.wait()
    of_gain.wait()
    tokens = tokens_ref[...].astype(jnp.float32)
    normed = rms_scale(tokens, mix_gain[...]).astype(jnp.bfloat16)
    of_bound.wait()
    bound = bound_ref[...]
    of_wf.wait()
    forget_pre = dot(normed, wf[...])
    forget = bound + (1.0 - bound) * sigmoid(forget_pre)
    key = (1.0 - bound) * sigmoid(-forget_pre)
    forget_ref[...] = forget
    key_ref[...] = key
    of_wq.wait()
    query = silu(dot(normed, wq[...]))
    of_wi.wait()
    input_val = dot(normed, wi[...])
    input_ref[...] = input_val
    forget_query = forget * query
    key_query = key * query
    columns = [forget_query[:, h * width : (h + 1) * width] for h in range(heads)]
    rows_left = width - seqs * heads
    if rows_left:
        columns.append(jnp.zeros((rows_left, width), jnp.float32))
    turned = jnp.concatenate(columns, axis=0).T
    of_wg.wait()
    gate = silu(dot(normed, wg[...]))
    of_head.wait()
    done = []
    for h in range(heads):
        of_state[h].wait()
        for s in range(seqs):
            at = h * seqs + s
            readout_ref[s : s + 1, :] = jnp.sum(
                state[h, s] * turned[:, at : at + 1], axis=0, keepdims=True
            )
        here = slice(h * width, (h + 1) * width)
        fresh = jnp.sum(key_query[:, here], axis=-1, keepdims=True) * input_val[:, here]
        readout = readout_ref[...] + fresh
        done.append((rms_scale(readout, head_gain[...]) * gate[:, here]).astype(jnp.bfloat16))
    of_wm.wait()
    part_ref[...] = dot(jnp.concatenate(done, axis=1), wm[...]).astype(jnp.bfloat16)


def mixer(tokens, mix_gain, head_gain, bound, wf, wq, wi, wg, state, wm):
    seqs, heads, width, _ = state.shape
    wide = jax.ShapeDtypeStruct((seqs, heads * width), jnp.float32)
    sources = (tokens, mix_gain[None], bound[None], wf, wq, wi, wg, head_gain[None], state, wm)
    held = [pltpu.VMEM(w.shape, w.dtype) for w in sources]
    held[8] = pltpu.VMEM((heads, seqs, width, width), jnp.float32)
    return pl.pallas_call(
        mixer_kernel,
        out_shape=(jax.ShapeDtypeStruct((seqs, wm.shape[1]), jnp.bfloat16), wide, wide, wide),
        in_specs=[HBM] * len(sources),
        out_specs=(VMEM,) * 4,
        scratch_shapes=held
        + [
            pltpu.VMEM((seqs, width), jnp.float32),
            pltpu.SemaphoreType.DMA((len(sources) - 1 + heads,)),
        ],
        cost_estimate=pl.CostEstimate(
            flops=40_000_000_000, bytes_accessed=16 << 20, transcendentals=0
        ),
        compiler_params=pltpu.CompilerParams(vmem_limit_bytes=20 << 20),
        name="mixer",
    )(*in_hbm(*sources))


def expert_kernel(x_ref, *refs):
    sources, out_ref, weights, sems = refs[:6], refs[6], refs[7:13], refs[13]
    copies = [None] * 6
    for i in (0, 1, 3, 4, 2, 5):
        copies[i] = pltpu.make_async_copy(sources[i], weights[i], sems.at[i])
        copies[i].start()
    x = x_ref[...]
    hidden = []
    for i in range(2):
        copies[3 * i].wait()
        gate = silu(dot(x, weights[3 * i][...]))
        copies[3 * i + 1].wait()
        hidden.append((gate * dot(x, weights[3 * i + 1][...])).astype(jnp.bfloat16))
    copies[2].wait()
    copies[5].wait()
    blocks, rows, width = out_ref.shape
    for t in range(2):
        here = slice(t * width, (t + 1) * width)
        total = dot(hidden[0], weights[2][:, here]) + dot(hidden[1], weights[5][:, here])
        total = total.astype(jnp.bfloat16)
        for c in range(blocks // 2):
            out_ref[2 * c + t] = total[c * rows : (c + 1) * rows]


def expert(x, weights, out_shape):
    return pl.pallas_call(
        expert_kernel,
        out_shape=jax.ShapeDtypeStruct(out_shape, jnp.bfloat16),
        in_specs=[VMEM] + [HBM] * 6,
        out_specs=VMEM,
        scratch_shapes=[pltpu.VMEM(w.shape, w.dtype) for w in weights]
        + [pltpu.SemaphoreType.DMA((6,))],
        compiler_params=pltpu.CompilerParams(vmem_limit_bytes=12 << 20),
        name="expert",
    )(x, *in_hbm(*weights))


def combine_kernel(returned_ref, weight_ref, own_ref, other_ref):
    blocks, rows, _ = returned_ref.shape
    half_rows = rows // 2
    for t in range(2):
        total = 0.0
        for at in range(t, blocks, 2):
            total = total + weight_ref[:, at : at + 1] * returned_ref[at].astype(jnp.float32)
        here = slice(t * half_rows, (t + 1) * half_rows)
        own_ref[here] = total[:half_rows]
        other_ref[here] = total[half_rows:].astype(jnp.bfloat16)


def combine(returned, weight):
    _, rows, width = returned.shape
    return pl.pallas_call(
        combine_kernel,
        out_shape=(
            jax.ShapeDtypeStruct((rows, width), jnp.float32),
            jax.ShapeDtypeStruct((rows, width), jnp.bfloat16),
        ),
        in_specs=[VMEM] * 2,
        out_specs=(VMEM,) * 2,
        compiler_params=pltpu.CompilerParams(vmem_limit_bytes=4 << 20),
        name="combine",
    )(returned, weight)


def local(
    tokens,
    state,
    mix_gain,
    moe_gain,
    head_gain,
    w_forget,
    w_query,
    w_input,
    w_outgate,
    lower_bound,
    w_mix_out,
    routes,
    route_scores,
    expert_gate,
    expert_up,
    expert_down,
    shared_gate,
    shared_up,
    shared_down,
):
    seqs_here, full_width = tokens.shape
    heads_here = state.shape[1]
    key_width = state.shape[2]
    n_ep = lax.axis_size("ep")
    n_tp = lax.axis_size("tp")
    tp_index = lax.axis_index("tp")
    half_width = full_width // n_tp
    half_rows = seqs_here // n_tp

    mix_part, forget, key_gate, input_val = mixer(
        tokens,
        mix_gain,
        head_gain,
        lower_bound,
        w_forget,
        w_query,
        w_input,
        w_outgate,
        state,
        w_mix_out,
    )
    by_head = (seqs_here, heads_here, key_width)
    new_state = (
        forget.reshape(by_head)[..., None] * state
        + key_gate.reshape(by_head)[..., None] * input_val.reshape(by_head)[:, :, None, :]
    )
    mixer_out = mix_part.astype(jnp.float32) + swap(mix_part).astype(jnp.float32)
    residual = tokens.astype(jnp.float32) + mixer_out.astype(jnp.bfloat16).astype(jnp.float32)
    moe_rows = rms_scale(residual, moe_gain).astype(jnp.bfloat16)

    half_ep = n_ep // 2
    halves = [list(range(half_ep)), list(range(half_ep, n_ep))]
    device_halves = [list(range(half_ep * n_tp)), list(range(half_ep * n_tp, n_ep * n_tp))]

    def across(values):
        return lax.ppermute(values, "ep", [(i, (i + half_ep) % n_ep) for i in range(n_ep)])

    own_rows = lax.dynamic_slice_in_dim(moe_rows, tp_index * half_rows, half_rows, 0)
    both_rows = jnp.concatenate([own_rows, across(own_rows)], axis=0)
    outgoing = jnp.broadcast_to(both_rows[None], (half_ep, seqs_here, full_width))
    own = (expert_gate[0], expert_up[0], expert_down[0])
    *own_late, outgoing = lax.optimization_barrier((*own, outgoing))
    other = tuple(swap(w) for w in own_late)
    arrived = lax.all_to_all(outgoing, "ep", 0, 0, axis_index_groups=halves)
    arrived = arrived.reshape(half_ep * seqs_here, full_width)

    weights = route_scores / jnp.sum(route_scores, axis=-1, keepdims=True) * routed_scale
    chosen = routes[:, :, None] == jnp.arange(n_ep, dtype=jnp.int32)[None, None, :]
    expert_weight = jnp.sum(jnp.where(chosen, weights[:, :, None], 0.0), axis=1)
    expert_weight = expert_weight.reshape(n_tp, half_rows, 2, half_ep)
    which = lax.axis_index("ep") // half_ep
    near = lax.dynamic_index_in_dim(expert_weight, which, 2, keepdims=False)
    far = lax.dynamic_index_in_dim(expert_weight, 1 - which, 2, keepdims=False)
    far = across(far)
    block_weight = jnp.stack([near, far], axis=0).transpose(0, 2, 3, 1)
    block_weight = block_weight.reshape(seqs_here, half_ep * n_tp)

    shared_hidden = (
        jax.nn.silu(dot(moe_rows, shared_gate)) * dot(moe_rows, shared_up)
    ).astype(jnp.bfloat16)
    shared_part = dot(shared_hidden, shared_down).astype(jnp.bfloat16)
    own_start = tp_index * half_width
    other_start = (1 - tp_index) * half_width
    shared_own = lax.dynamic_slice_in_dim(shared_part, own_start, half_width, 1)
    shared_sent = lax.dynamic_slice_in_dim(shared_part, other_start, half_width, 1)
    shared_out = shared_own.astype(jnp.float32) + swap(shared_sent).astype(jnp.float32)

    leaving = expert(arrived, own + other, (half_ep * n_tp, seqs_here, half_width))
    returned = lax.all_to_all(
        leaving, ("ep", "tp"), 0, 0, axis_index_groups=device_halves
    )
    routed_own, routed_other = combine(returned, block_weight)
    routed = routed_own + across(routed_other).astype(jnp.float32)
    residual_half = lax.dynamic_slice_in_dim(residual, own_start, half_width, 1)
    layer_out = (residual_half + routed + shared_out).astype(jnp.bfloat16)
    return (layer_out, new_state)


def solution(mesh):
    return jax.shard_map(
        local,
        mesh=mesh,
        in_specs=(
            P("ep", None),
            P("ep", "tp", None, None),
            P(),
            P(),
            P(),
            P(None, "tp"),
            P(None, "tp"),
            P(None, "tp"),
            P(None, "tp"),
            P("tp"),
            P("tp", None),
            P("ep", None),
            P("ep", None),
            P("ep", None, "tp"),
            P("ep", None, "tp"),
            P("ep", "tp", None),
            P(None, "tp"),
            P(None, "tp"),
            P("tp", None),
        ),
        out_specs=(P("ep", "tp"), P("ep", "tp", None, None)),
        check_vma=False,
    )
```

```python
import jax
import jax.numpy as jnp
from jax import lax
from jax.experimental import pallas as pl
from jax.experimental.pallas import tpu as pltpu
from jax.sharding import PartitionSpec as P


epsilon = 1e-06
routed_scale = 2.5
HBM = pl.BlockSpec(memory_space=pltpu.HBM)
VMEM = pl.BlockSpec(memory_space=pltpu.VMEM)


def rms_scale(values, gain):
    return values * lax.rsqrt(jnp.mean(values * values, axis=-1, keepdims=True) + epsilon) * gain


def dot(a, b):
    return jnp.dot(a, b, preferred_element_type=jnp.float32)


def silu(values):
    return values / (1.0 + jnp.exp(-values))


def sigmoid(values):
    return 1.0 / (1.0 + jnp.exp(-values))


def swap(values):
    return lax.ppermute(values, "tp", [(0, 1), (1, 0)])


def in_hbm(*values):
    return tuple(pltpu.with_memory_space_constraint(v, pltpu.HBM) for v in values)


def turned(values, heads):
    rows, width = values.shape[0], values.shape[1] // heads
    parts = [values[:, h * width : (h + 1) * width] for h in range(heads)]
    if width > rows * heads:
        parts.append(jnp.zeros((width - rows * heads, width), jnp.float32))
    return jnp.concatenate(parts, axis=0).T


def mixer_kernel(*refs):
    sources, refs = refs[:10], refs[10:]
    part_ref, forget_ref, key_ref, input_ref = refs[:4]
    targets, readout_ref, sems = refs[4:14], refs[14], refs[15]
    tokens_ref, mix_gain, bound_ref, wf, wq, wi, wg, head_gain, state, wm = targets
    state_hbm = sources[8]
    heads, seqs, width, _ = state.shape
    copies = []

    def start(source, target):
        copies.append(pltpu.make_async_copy(source, target, sems.at[len(copies)]))
        copies[-1].start()

    for i in range(8):
        start(sources[i], targets[i])
    for h in range(heads):
        start(state_hbm.at[:, h], state.at[h])
        if h == heads - 2:
            start(sources[9], wm)
    of_tokens, of_gain, of_bound, of_wf, of_wq, of_wi, of_wg, of_head, *of_state = copies
    of_wm = of_state.pop(heads - 1)

    of_tokens.wait()
    of_gain.wait()
    tokens = tokens_ref[...].astype(jnp.float32)
    normed = rms_scale(tokens, mix_gain[...]).astype(jnp.bfloat16)
    of_bound.wait()
    bound = bound_ref[...]
    of_wf.wait()
    forget_pre = dot(normed, wf[...])
    forget = bound + (1.0 - bound) * sigmoid(forget_pre)
    key = (1.0 - bound) * sigmoid(-forget_pre)
    forget_ref[...] = forget
    key_ref[...] = key
    of_wq.wait()
    query = silu(dot(normed, wq[...]))
    of_wi.wait()
    input_val = dot(normed, wi[...])
    input_ref[...] = input_val
    key_query = key * query

    columns = turned(forget * query, heads)
    of_wg.wait()
    gate = silu(dot(normed, wg[...]))
    of_head.wait()
    done = []
    for h in range(heads):
        of_state[h].wait()
        for s in range(seqs):
            at = h * seqs + s
            readout_ref[s : s + 1, :] = jnp.sum(
                state[h, s] * columns[:, at : at + 1], axis=0, keepdims=True
            )
        here = slice(h * width, (h + 1) * width)
        fresh = jnp.sum(key_query[:, here], axis=-1, keepdims=True) * input_val[:, here]
        readout = readout_ref[...] + fresh
        done.append((rms_scale(readout, head_gain[...]) * gate[:, here]).astype(jnp.bfloat16))
    of_wm.wait()
    part_ref[...] = dot(jnp.concatenate(done, axis=1), wm[...]).astype(jnp.bfloat16)


def mixer(tokens, mix_gain, head_gain, bound, wf, wq, wi, wg, state, wm):
    seqs, heads, width, _ = state.shape
    wide = jax.ShapeDtypeStruct((seqs, heads * width), jnp.float32)
    sources = (tokens, mix_gain[None], bound[None], wf, wq, wi, wg, head_gain[None], state, wm)
    held = [pltpu.VMEM(w.shape, w.dtype) for w in sources]
    held[8] = pltpu.VMEM((heads, seqs, width, width), jnp.float32)
    return pl.pallas_call(
        mixer_kernel,
        out_shape=(jax.ShapeDtypeStruct((seqs, wm.shape[1]), jnp.bfloat16), wide, wide, wide),
        in_specs=[HBM] * len(sources),
        out_specs=(VMEM,) * 4,
        scratch_shapes=held
        + [
            pltpu.VMEM((seqs, width), jnp.float32),
            pltpu.SemaphoreType.DMA((len(sources) - 1 + heads,)),
        ],
        cost_estimate=pl.CostEstimate(
            flops=40_000_000_000, bytes_accessed=16 << 20, transcendentals=0
        ),
        compiler_params=pltpu.CompilerParams(vmem_limit_bytes=20 << 20),
        name="mixer",
    )(*in_hbm(*sources))


def beside_kernel(forget_ref, key_ref, input_ref, gate_hbm, up_hbm, state_hbm, *refs):
    gate_ref, up_ref, fresh_hbm, old, fresh, in_sems, out_sems = refs
    heads, pieces, rows = old.shape[:3]
    width = old.shape[-1]
    chunks = [(h, p) for h in range(heads) for p in range(pieces)]

    def of(ref, h, p):
        return ref.at[p * rows : (p + 1) * rows, h]

    reads = [
        pltpu.make_async_copy(of(state_hbm, *c), old.at[c], in_sems.at[i])
        for i, c in enumerate(chunks)
    ]
    writes = [
        pltpu.make_async_copy(fresh.at[c], of(fresh_hbm, *c), out_sems.at[i])
        for i, c in enumerate(chunks)
    ]
    weights = [
        pltpu.make_async_copy(gate_hbm, gate_ref, in_sems.at[len(chunks)]),
        pltpu.make_async_copy(up_hbm, up_ref, in_sems.at[len(chunks) + 1]),
    ]
    for copy in reads + weights:
        copy.start()
    forget, key = turned(forget_ref[...], heads), turned(key_ref[...], heads)
    for i, (h, p) in enumerate(chunks):
        reads[i].wait()
        for r in range(rows):
            s = p * rows + r
            at = h * pieces * rows + s
            written = input_ref[s : s + 1, h * width : (h + 1) * width]
            fresh[h, p, r] = (
                forget[:, at : at + 1] * old[h, p, r] + key[:, at : at + 1] * written
            )
        writes[i].start()
    for copy in weights + writes:
        copy.wait()


def beside(forget, key, input_val, gate, up, state):
    seqs, heads, width, _ = state.shape
    pieces = 2 if seqs % 2 == 0 else 1
    buffer = pltpu.VMEM((heads, pieces, seqs // pieces, width, width), jnp.float32)
    return pl.pallas_call(
        beside_kernel,
        out_shape=(
            pltpu.VMEM(gate.shape, gate.dtype),
            pltpu.VMEM(up.shape, up.dtype),
            jax.ShapeDtypeStruct(state.shape, jnp.float32),
        ),
        in_specs=[VMEM] * 3 + [HBM] * 3,
        out_specs=(VMEM, VMEM, HBM),
        scratch_shapes=[
            buffer,
            buffer,
            pltpu.SemaphoreType.DMA((heads * pieces + 2,)),
            pltpu.SemaphoreType.DMA((heads * pieces,)),
        ],
        compiler_params=pltpu.CompilerParams(vmem_limit_bytes=12 << 20),
        name="beside",
    )(forget, key, input_val, *in_hbm(gate, up, state))


def expert_kernel(x_ref, gate_ref, up_ref, *refs):
    sources, out_hbm, weights, out_ref, sems = refs[:4], refs[4], refs[5:9], refs[9], refs[10]
    copies = [pltpu.make_async_copy(sources[i], weights[i], sems.at[i]) for i in range(4)]
    for copy in copies:
        copy.start()
    x = x_ref[...]
    near = (silu(dot(x, gate_ref[...])) * dot(x, up_ref[...])).astype(jnp.bfloat16)
    copies[0].wait()
    gate = silu(dot(x, weights[0][...]))
    copies[1].wait()
    far = (gate * dot(x, weights[1][...])).astype(jnp.bfloat16)
    copies[2].wait()
    copies[3].wait()
    parts, width = 2, out_ref.shape[1]
    leaving = []
    for p in range(parts):
        here = slice(p * width // parts, (p + 1) * width // parts)
        total = dot(near, weights[2][:, here]) + dot(far, weights[3][:, here])
        out_ref[:, here] = total.astype(jnp.bfloat16)
        leaving.append(
            pltpu.make_async_copy(out_ref.at[:, here], out_hbm.at[:, here], sems.at[4 + p])
        )
        leaving[-1].start()
    for copy in leaving:
        copy.wait()


def expert(x, own, other):
    gate, up, down = own
    sources = (other[0], other[1], down, other[2])
    return pl.pallas_call(
        expert_kernel,
        out_shape=jax.ShapeDtypeStruct(x.shape, jnp.bfloat16),
        in_specs=[VMEM] * 3 + [HBM] * 4,
        out_specs=HBM,
        scratch_shapes=[pltpu.VMEM(w.shape, w.dtype) for w in sources]
        + [pltpu.VMEM(x.shape, x.dtype), pltpu.SemaphoreType.DMA((6,))],
        compiler_params=pltpu.CompilerParams(vmem_limit_bytes=10 << 20),
        name="expert",
    )(
        x,
        pltpu.with_memory_space_constraint(gate, pltpu.VMEM),
        pltpu.with_memory_space_constraint(up, pltpu.VMEM),
        *in_hbm(*sources),
    )


def shared_kernel(x_ref, *refs):
    sources, out_ref, weights, sems = refs[:3], refs[3], refs[4:7], refs[7]
    copies = [pltpu.make_async_copy(sources[i], weights[i], sems.at[i]) for i in range(3)]
    for copy in copies:
        copy.start()
    x = x_ref[...]
    copies[0].wait()
    gate = silu(dot(x, weights[0][...]))
    copies[1].wait()
    hidden = (gate * dot(x, weights[1][...])).astype(jnp.bfloat16)
    copies[2].wait()
    out_ref[...] = dot(hidden, weights[2][...]).astype(jnp.bfloat16)


def shared_expert(x, *weights):
    return pl.pallas_call(
        shared_kernel,
        out_shape=jax.ShapeDtypeStruct(x.shape, jnp.bfloat16),
        in_specs=[VMEM] + [HBM] * 3,
        out_specs=VMEM,
        scratch_shapes=[pltpu.VMEM(w.shape, w.dtype) for w in weights]
        + [pltpu.SemaphoreType.DMA((3,))],
        cost_estimate=pl.CostEstimate(
            flops=10_000_000_000, bytes_accessed=3 << 20, transcendentals=0
        ),
        compiler_params=pltpu.CompilerParams(vmem_limit_bytes=6 << 20),
        name="shared_expert",
    )(x, *in_hbm(*weights))


def combine_kernel(returned_ref, weight_ref, kept_ref, far_ref):
    blocks, rows, _ = returned_ref.shape
    total = 0.0
    for e in range(blocks):
        total = total + weight_ref[:, e : e + 1] * returned_ref[e].astype(jnp.float32)
    kept_ref[...] = total[: rows // 2]
    far_ref[...] = total[rows // 2 :].astype(jnp.bfloat16)


def combine(returned, weight):
    _, rows, width = returned.shape
    shape = (rows // 2, width)
    return pl.pallas_call(
        combine_kernel,
        out_shape=(
            jax.ShapeDtypeStruct(shape, jnp.float32),
            jax.ShapeDtypeStruct(shape, jnp.bfloat16),
        ),
        in_specs=[VMEM] * 2,
        out_specs=(VMEM,) * 2,
        compiler_params=pltpu.CompilerParams(vmem_limit_bytes=4 << 20),
        name="combine",
    )(returned, weight)


def local(
    tokens,
    state,
    mix_gain,
    moe_gain,
    head_gain,
    w_forget,
    w_query,
    w_input,
    w_outgate,
    lower_bound,
    w_mix_out,
    routes,
    route_scores,
    expert_gate,
    expert_up,
    expert_down,
    shared_gate,
    shared_up,
    shared_down,
):
    seqs_here, full_width = tokens.shape
    n_ep = lax.axis_size("ep")
    n_tp = lax.axis_size("tp")
    tp_index = lax.axis_index("tp")
    half_width = full_width // n_tp
    half_rows = seqs_here // n_tp

    mix_part, forget, key_gate, input_val = mixer(
        tokens,
        mix_gain,
        head_gain,
        lower_bound,
        w_forget,
        w_query,
        w_input,
        w_outgate,
        state,
        w_mix_out,
    )
    mixer_out = mix_part.astype(jnp.float32) + swap(mix_part).astype(jnp.float32)
    residual = tokens.astype(jnp.float32) + mixer_out.astype(jnp.bfloat16).astype(jnp.float32)
    moe_rows = rms_scale(residual, moe_gain).astype(jnp.bfloat16)

    half_ep = n_ep // 2
    halves = [list(range(half_ep)), list(range(half_ep, n_ep))]

    def across(values):
        return lax.ppermute(values, "ep", [(i, (i + half_ep) % n_ep) for i in range(n_ep)])

    own_rows = lax.dynamic_slice_in_dim(moe_rows, tp_index * half_rows, half_rows, 0)
    far_rows = across(own_rows)
    both_rows = jnp.concatenate([own_rows, far_rows], axis=0)
    outgoing = jnp.broadcast_to(both_rows[None], (half_ep, seqs_here, full_width))
    own = (expert_gate[0], expert_up[0], expert_down[0])
    *own_late, _ = lax.optimization_barrier((*own, own_rows))
    other = tuple(swap(w) for w in own_late)
    arrived = lax.all_to_all(outgoing, "ep", 0, 0, axis_index_groups=halves)
    arrived = arrived.reshape(half_ep * seqs_here, full_width)

    weights = route_scores / jnp.sum(route_scores, axis=-1, keepdims=True) * routed_scale
    chosen = routes[:, :, None] == jnp.arange(n_ep, dtype=jnp.int32)[None, None, :]
    expert_weight = jnp.sum(jnp.where(chosen, weights[:, :, None], 0.0), axis=1)
    expert_weight = lax.dynamic_slice_in_dim(expert_weight, tp_index * half_rows, half_rows, 0)
    expert_weight = expert_weight.reshape(half_rows, 2, half_ep)
    which = lax.axis_index("ep") // half_ep
    near = lax.dynamic_index_in_dim(expert_weight, which, 1, keepdims=False)
    far = lax.dynamic_index_in_dim(expert_weight, 1 - which, 1, keepdims=False)
    far = across(far)
    block_weight = jnp.concatenate([near, far], axis=0)

    shared_part = shared_expert(moe_rows, shared_gate, shared_up, shared_down)
    own_start = tp_index * half_width
    other_start = (1 - tp_index) * half_width
    shared_own = lax.dynamic_slice_in_dim(shared_part, own_start, half_width, 1)
    shared_sent = lax.dynamic_slice_in_dim(shared_part, other_start, half_width, 1)
    shared_got = swap(shared_sent)
    shared_out = shared_own.astype(jnp.float32) + shared_got.astype(jnp.float32)

    *ready, new_state = beside(forget, key_gate, input_val, own[0], own[1], state)
    leaving = expert(arrived, (*ready, own[2]), other).reshape(half_ep, seqs_here, full_width)
    returned = lax.all_to_all(leaving, "ep", 0, 0, axis_index_groups=halves)
    kept, far = combine(returned, block_weight)
    far = across(far)
    own_block = kept + far.astype(jnp.float32)
    keeping = lax.dynamic_slice_in_dim(own_block, own_start, half_width, 1)
    giving = lax.dynamic_slice_in_dim(own_block, other_start, half_width, 1)
    other_block = swap(giving.astype(jnp.bfloat16)).astype(jnp.float32)
    first = tp_index == 0
    routed = jnp.concatenate(
        [jnp.where(first, keeping, other_block), jnp.where(first, other_block, keeping)],
        axis=0,
    )
    residual_half = lax.dynamic_slice_in_dim(residual, own_start, half_width, 1)
    layer_out = (residual_half + routed + shared_out).astype(jnp.bfloat16)
    return (layer_out, new_state)


def solution(mesh):
    return jax.shard_map(
        local,
        mesh=mesh,
        in_specs=(
            P("ep", None),
            P("ep", "tp", None, None),
            P(),
            P(),
            P(),
            P(None, "tp"),
            P(None, "tp"),
            P(None, "tp"),
            P(None, "tp"),
            P("tp"),
            P("tp", None),
            P("ep", None),
            P("ep", None),
            P("ep", None, "tp"),
            P("ep", None, "tp"),
            P("ep", "tp", None),
            P(None, "tp"),
            P(None, "tp"),
            P("tp", None),
        ),
        out_specs=(P("ep", "tp"), P("ep", "tp", None, None)),
        check_vma=False,
    )
```

```python
import jax
import jax.numpy as jnp
from jax import lax
from jax.experimental import pallas as pl
from jax.experimental.pallas import tpu as pltpu
from jax.sharding import PartitionSpec as P


epsilon = 1e-06
routed_scale = 2.5
HBM = pl.BlockSpec(memory_space=pltpu.HBM)
VMEM = pl.BlockSpec(memory_space=pltpu.VMEM)


def rms_scale(values, gain):
    return values * lax.rsqrt(jnp.mean(values * values, axis=-1, keepdims=True) + epsilon) * gain


def dot(a, b):
    return jnp.dot(a, b, preferred_element_type=jnp.float32)


def silu(values):
    return values / (1.0 + jnp.exp(-values))


def sigmoid(values):
    return 1.0 / (1.0 + jnp.exp(-values))


def swap(values):
    return lax.ppermute(values, "tp", [(0, 1), (1, 0)])


def in_hbm(*values):
    return tuple(pltpu.with_memory_space_constraint(v, pltpu.HBM) for v in values)


def turned(values, heads):
    rows, width = values.shape[0], values.shape[1] // heads
    parts = [values[:, h * width : (h + 1) * width] for h in range(heads)]
    if width > rows * heads:
        parts.append(jnp.zeros((width - rows * heads, width), jnp.float32))
    return jnp.concatenate(parts, axis=0).T


def mixer_kernel(*refs):
    sources, refs = refs[:10], refs[10:]
    part_ref, forget_ref, key_ref, input_ref = refs[:4]
    targets, readout_ref, sems = refs[4:14], refs[14], refs[15]
    tokens_ref, mix_gain, bound_ref, wf, wq, wi, wg, head_gain, state, wm = targets
    state_hbm, wm_hbm = sources[8], sources[9]
    heads, seqs, width, _ = state.shape
    half = wm.shape[0] // 2
    copies = {}

    def start(name, source, target):
        copies[name] = pltpu.make_async_copy(source, target, sems.at[len(copies)])
        copies[name].start()

    def start_state(h):
        start(h, state_hbm.at[:, h], state.at[h])

    def start_mix(name, at):
        start(name, wm_hbm.at[at : at + half], wm.at[at : at + half])

    for name, i in (("tokens", 0), ("gain", 1), ("bound", 2), ("head", 7), ("f", 3), ("q", 4)):
        start(name, sources[i], targets[i])
    for h in range(heads):
        start_state(h)
    start("i", sources[5], wi)
    start("g", sources[6], wg)
    start_mix("m0", 0)
    start_mix("m1", half)
    copies["tokens"].wait()
    copies["gain"].wait()
    tokens = tokens_ref[...].astype(jnp.float32)
    normed = rms_scale(tokens, mix_gain[...]).astype(jnp.bfloat16)
    copies["bound"].wait()
    bound = bound_ref[...]
    copies["f"].wait()
    forget_pre = dot(normed, wf[...])
    forget = bound + (1.0 - bound) * sigmoid(forget_pre)
    key = (1.0 - bound) * sigmoid(-forget_pre)
    forget_ref[...] = forget
    key_ref[...] = key
    copies["q"].wait()
    query = silu(dot(normed, wq[...]))
    key_query = key * query
    columns = turned(forget * query, heads)

    def read_out(h):
        copies[h].wait()
        for s in range(seqs):
            at = h * seqs + s
            readout_ref[h, s : s + 1, :] = jnp.sum(
                state[h, s] * columns[:, at : at + 1], axis=0, keepdims=True
            )

    for h in range(heads):
        read_out(h)
    copies["i"].wait()
    input_val = dot(normed, wi[...])
    input_ref[...] = input_val
    copies["g"].wait()
    gate = silu(dot(normed, wg[...]))
    copies["head"].wait()
    done = []
    for h in range(heads):
        here = slice(h * width, (h + 1) * width)
        fresh = jnp.sum(key_query[:, here], axis=-1, keepdims=True) * input_val[:, here]
        readout = readout_ref[h] + fresh
        done.append((rms_scale(readout, head_gain[...]) * gate[:, here]).astype(jnp.bfloat16))
    done = jnp.concatenate(done, axis=1)
    copies["m0"].wait()
    copies["m1"].wait()
    part_ref[...] = dot(done, wm[...]).astype(jnp.bfloat16)


def mixer(tokens, mix_gain, head_gain, bound, wf, wq, wi, wg, state, wm):
    seqs, heads, width, _ = state.shape
    wide = jax.ShapeDtypeStruct((seqs, heads * width), jnp.float32)
    sources = (tokens, mix_gain[None], bound[None], wf, wq, wi, wg, head_gain[None], state, wm)
    held = [pltpu.VMEM(w.shape, w.dtype) for w in sources]
    held[8] = pltpu.VMEM((heads, seqs, width, width), jnp.float32)
    return pl.pallas_call(
        mixer_kernel,
        out_shape=(jax.ShapeDtypeStruct((seqs, wm.shape[1]), jnp.bfloat16), wide, wide, wide),
        in_specs=[HBM] * len(sources),
        out_specs=(VMEM,) * 4,
        scratch_shapes=held
        + [
            pltpu.VMEM((heads, seqs, width), jnp.float32),
            pltpu.SemaphoreType.DMA((len(sources) + heads,)),
        ],
        cost_estimate=pl.CostEstimate(
            flops=40_000_000_000, bytes_accessed=16 << 20, transcendentals=0
        ),
        compiler_params=pltpu.CompilerParams(vmem_limit_bytes=20 << 20),
        name="mixer",
    )(*in_hbm(*sources))


def beside_kernel(forget_ref, key_ref, input_ref, gate_hbm, up_hbm, state_hbm, *refs):
    gate_ref, up_ref, fresh_hbm, old, fresh, in_sems, out_sems = refs
    heads, pieces, rows = old.shape[:3]
    width = old.shape[-1]
    chunks = [(h, p) for h in range(heads) for p in range(pieces)]

    def of(ref, h, p):
        return ref.at[p * rows : (p + 1) * rows, h]

    reads = [
        pltpu.make_async_copy(of(state_hbm, *c), old.at[c], in_sems.at[i])
        for i, c in enumerate(chunks)
    ]
    writes = [
        pltpu.make_async_copy(fresh.at[c], of(fresh_hbm, *c), out_sems.at[i])
        for i, c in enumerate(chunks)
    ]
    weights = [
        pltpu.make_async_copy(gate_hbm, gate_ref, in_sems.at[len(chunks)]),
        pltpu.make_async_copy(up_hbm, up_ref, in_sems.at[len(chunks) + 1]),
    ]
    for copy in reads + weights:
        copy.start()
    forget, key = turned(forget_ref[...], heads), turned(key_ref[...], heads)
    for i, (h, p) in enumerate(chunks):
        reads[i].wait()
        for r in range(rows):
            s = p * rows + r
            at = h * pieces * rows + s
            written = input_ref[s : s + 1, h * width : (h + 1) * width]
            fresh[h, p, r] = (
                forget[:, at : at + 1] * old[h, p, r] + key[:, at : at + 1] * written
            )
        writes[i].start()
    for copy in weights + writes:
        copy.wait()


def beside(forget, key, input_val, gate, up, state):
    seqs, heads, width, _ = state.shape
    pieces = 2 if seqs % 2 == 0 else 1
    buffer = pltpu.VMEM((heads, pieces, seqs // pieces, width, width), jnp.float32)
    return pl.pallas_call(
        beside_kernel,
        out_shape=(
            pltpu.VMEM(gate.shape, gate.dtype),
            pltpu.VMEM(up.shape, up.dtype),
            jax.ShapeDtypeStruct(state.shape, jnp.float32),
        ),
        in_specs=[VMEM] * 3 + [HBM] * 3,
        out_specs=(VMEM, VMEM, HBM),
        scratch_shapes=[
            buffer,
            buffer,
            pltpu.SemaphoreType.DMA((heads * pieces + 2,)),
            pltpu.SemaphoreType.DMA((heads * pieces,)),
        ],
        compiler_params=pltpu.CompilerParams(vmem_limit_bytes=12 << 20),
        name="beside",
    )(forget, key, input_val, *in_hbm(gate, up, state))


def expert_kernel(x_ref, gate_ref, up_ref, *refs):
    sources, out_hbm, weights, out_ref, sems = refs[:4], refs[4], refs[5:9], refs[9], refs[10]
    copies = [pltpu.make_async_copy(sources[i], weights[i], sems.at[i]) for i in range(4)]
    for copy in copies:
        copy.start()
    x = x_ref[...]
    near = (silu(dot(x, gate_ref[...])) * dot(x, up_ref[...])).astype(jnp.bfloat16)
    copies[0].wait()
    gate = silu(dot(x, weights[0][...]))
    copies[1].wait()
    far = (gate * dot(x, weights[1][...])).astype(jnp.bfloat16)
    copies[2].wait()
    copies[3].wait()
    parts, width = 2, out_ref.shape[1]
    leaving = []
    for p in range(parts):
        here = slice(p * width // parts, (p + 1) * width // parts)
        total = dot(near, weights[2][:, here]) + dot(far, weights[3][:, here])
        out_ref[:, here] = total.astype(jnp.bfloat16)
        leaving.append(
            pltpu.make_async_copy(out_ref.at[:, here], out_hbm.at[:, here], sems.at[4 + p])
        )
        leaving[-1].start()
    for copy in leaving:
        copy.wait()


def expert(x, own, other):
    gate, up, down = own
    sources = (other[0], other[1], down, other[2])
    return pl.pallas_call(
        expert_kernel,
        out_shape=jax.ShapeDtypeStruct(x.shape, jnp.bfloat16),
        in_specs=[VMEM] * 3 + [HBM] * 4,
        out_specs=HBM,
        scratch_shapes=[pltpu.VMEM(w.shape, w.dtype) for w in sources]
        + [pltpu.VMEM(x.shape, x.dtype), pltpu.SemaphoreType.DMA((6,))],
        compiler_params=pltpu.CompilerParams(vmem_limit_bytes=10 << 20),
        name="expert",
    )(
        x,
        pltpu.with_memory_space_constraint(gate, pltpu.VMEM),
        pltpu.with_memory_space_constraint(up, pltpu.VMEM),
        *in_hbm(*sources),
    )


def shared_kernel(x_ref, *refs):
    sources, out_ref, weights, sems = refs[:3], refs[3], refs[4:7], refs[7]
    copies = [pltpu.make_async_copy(sources[i], weights[i], sems.at[i]) for i in range(3)]
    for copy in copies:
        copy.start()
    x = x_ref[...]
    copies[0].wait()
    gate = silu(dot(x, weights[0][...]))
    copies[1].wait()
    hidden = (gate * dot(x, weights[1][...])).astype(jnp.bfloat16)
    copies[2].wait()
    out_ref[...] = dot(hidden, weights[2][...]).astype(jnp.bfloat16)


def shared_expert(x, *weights):
    return pl.pallas_call(
        shared_kernel,
        out_shape=jax.ShapeDtypeStruct(x.shape, jnp.bfloat16),
        in_specs=[VMEM] + [HBM] * 3,
        out_specs=VMEM,
        scratch_shapes=[pltpu.VMEM(w.shape, w.dtype) for w in weights]
        + [pltpu.SemaphoreType.DMA((3,))],
        cost_estimate=pl.CostEstimate(
            flops=10_000_000_000, bytes_accessed=3 << 20, transcendentals=0
        ),
        compiler_params=pltpu.CompilerParams(vmem_limit_bytes=6 << 20),
        name="shared_expert",
    )(x, *in_hbm(*weights))


def combine_kernel(returned_ref, weight_ref, kept_ref, far_ref):
    blocks, rows, _ = returned_ref.shape
    total = 0.0
    for e in range(blocks):
        total = total + weight_ref[:, e : e + 1] * returned_ref[e].astype(jnp.float32)
    kept_ref[...] = total[: rows // 2]
    far_ref[...] = total[rows // 2 :].astype(jnp.bfloat16)


def combine(returned, weight):
    _, rows, width = returned.shape
    shape = (rows // 2, width)
    return pl.pallas_call(
        combine_kernel,
        out_shape=(
            jax.ShapeDtypeStruct(shape, jnp.float32),
            jax.ShapeDtypeStruct(shape, jnp.bfloat16),
        ),
        in_specs=[VMEM] * 2,
        out_specs=(VMEM,) * 2,
        compiler_params=pltpu.CompilerParams(vmem_limit_bytes=4 << 20),
        name="combine",
    )(returned, weight)


def local(
    tokens,
    state,
    mix_gain,
    moe_gain,
    head_gain,
    w_forget,
    w_query,
    w_input,
    w_outgate,
    lower_bound,
    w_mix_out,
    routes,
    route_scores,
    expert_gate,
    expert_up,
    expert_down,
    shared_gate,
    shared_up,
    shared_down,
):
    seqs_here, full_width = tokens.shape
    n_ep = lax.axis_size("ep")
    n_tp = lax.axis_size("tp")
    tp_index = lax.axis_index("tp")
    half_width = full_width // n_tp
    half_rows = seqs_here // n_tp

    mix_part, forget, key_gate, input_val = mixer(
        tokens,
        mix_gain,
        head_gain,
        lower_bound,
        w_forget,
        w_query,
        w_input,
        w_outgate,
        state,
        w_mix_out,
    )
    mixer_out = mix_part.astype(jnp.float32) + swap(mix_part).astype(jnp.float32)
    residual = tokens.astype(jnp.float32) + mixer_out.astype(jnp.bfloat16).astype(jnp.float32)
    moe_rows = rms_scale(residual, moe_gain).astype(jnp.bfloat16)

    half_ep = n_ep // 2
    halves = [list(range(half_ep)), list(range(half_ep, n_ep))]

    def across(values):
        return lax.ppermute(values, "ep", [(i, (i + half_ep) % n_ep) for i in range(n_ep)])

    own_rows = lax.dynamic_slice_in_dim(moe_rows, tp_index * half_rows, half_rows, 0)
    far_rows = across(own_rows)
    both_rows = jnp.concatenate([own_rows, far_rows], axis=0)
    outgoing = jnp.broadcast_to(both_rows[None], (half_ep, seqs_here, full_width))
    own = (expert_gate[0], expert_up[0], expert_down[0])
    *own_late, _ = lax.optimization_barrier((*own, own_rows))
    other = tuple(swap(w) for w in own_late)
    arrived = lax.all_to_all(outgoing, "ep", 0, 0, axis_index_groups=halves)
    arrived = arrived.reshape(half_ep * seqs_here, full_width)

    weights = route_scores / jnp.sum(route_scores, axis=-1, keepdims=True) * routed_scale
    chosen = routes[:, :, None] == jnp.arange(n_ep, dtype=jnp.int32)[None, None, :]
    expert_weight = jnp.sum(jnp.where(chosen, weights[:, :, None], 0.0), axis=1)
    expert_weight = lax.dynamic_slice_in_dim(expert_weight, tp_index * half_rows, half_rows, 0)
    expert_weight = expert_weight.reshape(half_rows, 2, half_ep)
    which = lax.axis_index("ep") // half_ep
    near = lax.dynamic_index_in_dim(expert_weight, which, 1, keepdims=False)
    far = lax.dynamic_index_in_dim(expert_weight, 1 - which, 1, keepdims=False)
    far = across(far)
    block_weight = jnp.concatenate([near, far], axis=0)

    shared_part = shared_expert(moe_rows, shared_gate, shared_up, shared_down)
    own_start = tp_index * half_width
    other_start = (1 - tp_index) * half_width
    shared_own = lax.dynamic_slice_in_dim(shared_part, own_start, half_width, 1)
    shared_sent = lax.dynamic_slice_in_dim(shared_part, other_start, half_width, 1)
    shared_got = swap(shared_sent)
    shared_out = shared_own.astype(jnp.float32) + shared_got.astype(jnp.float32)

    *ready, new_state = beside(forget, key_gate, input_val, own[0], own[1], state)
    leaving = expert(arrived, (*ready, own[2]), other).reshape(half_ep, seqs_here, full_width)
    returned = lax.all_to_all(leaving, "ep", 0, 0, axis_index_groups=halves)
    kept, far = combine(returned, block_weight)
    far = across(far)
    own_block = kept + far.astype(jnp.float32)
    keeping = lax.dynamic_slice_in_dim(own_block, own_start, half_width, 1)
    giving = lax.dynamic_slice_in_dim(own_block, other_start, half_width, 1)
    other_block = swap(giving.astype(jnp.bfloat16)).astype(jnp.float32)
    first = tp_index == 0
    routed = jnp.concatenate(
        [jnp.where(first, keeping, other_block), jnp.where(first, other_block, keeping)],
        axis=0,
    )
    residual_half = lax.dynamic_slice_in_dim(residual, own_start, half_width, 1)
    layer_out = (residual_half + routed + shared_out).astype(jnp.bfloat16)
    return (layer_out, new_state)


def solution(mesh):
    return jax.shard_map(
        local,
        mesh=mesh,
        in_specs=(
            P("ep", None),
            P("ep", "tp", None, None),
            P(),
            P(),
            P(),
            P(None, "tp"),
            P(None, "tp"),
            P(None, "tp"),
            P(None, "tp"),
            P("tp"),
            P("tp", None),
            P("ep", None),
            P("ep", None),
            P("ep", None, "tp"),
            P("ep", None, "tp"),
            P("ep", "tp", None),
            P(None, "tp"),
            P(None, "tp"),
            P("tp", None),
        ),
        out_specs=(P("ep", "tp"), P("ep", "tp", None, None)),
        check_vma=False,
    )
```

```python
import jax
import jax.numpy as jnp
from jax import lax
from jax.experimental import pallas as pl
from jax.experimental.pallas import tpu as pltpu
from jax.sharding import PartitionSpec as P


epsilon = 1e-06
routed_scale = 2.5
HBM = pl.BlockSpec(memory_space=pltpu.HBM)
VMEM = pl.BlockSpec(memory_space=pltpu.VMEM)


def rms_scale(values, gain):
    return values * lax.rsqrt(jnp.mean(values * values, axis=-1, keepdims=True) + epsilon) * gain


def dot(a, b):
    return jnp.dot(a, b, preferred_element_type=jnp.float32)


def silu(values):
    return values / (1.0 + jnp.exp(-values))


def sigmoid(values):
    return 1.0 / (1.0 + jnp.exp(-values))


def swap(values):
    return lax.ppermute(values, "tp", [(0, 1), (1, 0)])


def in_hbm(*values):
    return tuple(pltpu.with_memory_space_constraint(v, pltpu.HBM) for v in values)


def turned(values, heads):
    rows, width = values.shape[0], values.shape[1] // heads
    parts = [values[:, h * width : (h + 1) * width] for h in range(heads)]
    if width > rows * heads:
        parts.append(jnp.zeros((width - rows * heads, width), jnp.float32))
    return jnp.concatenate(parts, axis=0).T


def mixer_kernel(*refs):
    sources, refs = refs[:10], refs[10:]
    part_ref, forget_ref, key_ref, input_ref = refs[:4]
    targets, readout_ref, sems = refs[4:14], refs[14], refs[15]
    tokens_ref, mix_gain, bound_ref, wf, wq, wi, wg, head_gain, state, wm = targets
    state_hbm, wm_hbm = sources[8], sources[9]
    heads, seqs, width, _ = state.shape
    half = wm.shape[0] // 2
    copies = {}

    def start(name, source, target):
        copies[name] = pltpu.make_async_copy(source, target, sems.at[len(copies)])
        copies[name].start()

    def start_state(h):
        start(h, state_hbm.at[:, h], state.at[h])

    def start_mix(name, at):
        start(name, wm_hbm.at[at : at + half], wm.at[at : at + half])

    for name, i in (("tokens", 0), ("gain", 1), ("bound", 2), ("head", 7), ("f", 3), ("q", 4)):
        start(name, sources[i], targets[i])
    for h in range(heads):
        start_state(h)
    start("i", sources[5], wi)
    start("g", sources[6], wg)
    start_mix("m0", 0)
    start_mix("m1", half)
    copies["tokens"].wait()
    copies["gain"].wait()
    tokens = tokens_ref[...].astype(jnp.float32)
    normed = rms_scale(tokens, mix_gain[...]).astype(jnp.bfloat16)
    copies["bound"].wait()
    bound = bound_ref[...]
    copies["f"].wait()
    forget_pre = dot(normed, wf[...])
    forget = bound + (1.0 - bound) * sigmoid(forget_pre)
    key = (1.0 - bound) * sigmoid(-forget_pre)
    forget_ref[...] = forget
    key_ref[...] = key
    copies["q"].wait()
    query = silu(dot(normed, wq[...]))
    key_query = key * query
    columns = turned(forget * query, heads)

    def read_out(h):
        copies[h].wait()
        for s in range(seqs):
            at = h * seqs + s
            readout_ref[h, s : s + 1, :] = jnp.sum(
                state[h, s] * columns[:, at : at + 1], axis=0, keepdims=True
            )

    for h in range(heads):
        read_out(h)
    copies["i"].wait()
    input_val = dot(normed, wi[...])
    input_ref[...] = input_val
    copies["g"].wait()
    gate = silu(dot(normed, wg[...]))
    copies["head"].wait()
    done = []
    for h in range(heads):
        here = slice(h * width, (h + 1) * width)
        fresh = jnp.sum(key_query[:, here], axis=-1, keepdims=True) * input_val[:, here]
        readout = readout_ref[h] + fresh
        done.append((rms_scale(readout, head_gain[...]) * gate[:, here]).astype(jnp.bfloat16))
    done = jnp.concatenate(done, axis=1)
    copies["m0"].wait()
    copies["m1"].wait()
    part_ref[...] = dot(done, wm[...]).astype(jnp.bfloat16)


def mixer(tokens, mix_gain, head_gain, bound, wf, wq, wi, wg, state, wm):
    seqs, heads, width, _ = state.shape
    wide = jax.ShapeDtypeStruct((seqs, heads * width), jnp.float32)
    sources = (tokens, mix_gain[None], bound[None], wf, wq, wi, wg, head_gain[None], state, wm)
    held = [pltpu.VMEM(w.shape, w.dtype) for w in sources]
    held[8] = pltpu.VMEM((heads, seqs, width, width), jnp.float32)
    return pl.pallas_call(
        mixer_kernel,
        out_shape=(jax.ShapeDtypeStruct((seqs, wm.shape[1]), jnp.bfloat16), wide, wide, wide),
        in_specs=[HBM] * len(sources),
        out_specs=(VMEM,) * 4,
        scratch_shapes=held
        + [
            pltpu.VMEM((heads, seqs, width), jnp.float32),
            pltpu.SemaphoreType.DMA((len(sources) + heads,)),
        ],
        cost_estimate=pl.CostEstimate(
            flops=40_000_000_000, bytes_accessed=16 << 20, transcendentals=0
        ),
        compiler_params=pltpu.CompilerParams(vmem_limit_bytes=20 << 20),
        name="mixer",
    )(*in_hbm(*sources))


def beside_kernel(forget_ref, key_ref, input_ref, gate_hbm, up_hbm, state_hbm, *refs):
    gate_ref, up_ref, fresh_hbm, old, fresh, in_sems, out_sems = refs
    heads, pieces, rows = old.shape[:3]
    width = old.shape[-1]
    chunks = [(h, p) for h in range(heads) for p in range(pieces)]

    def of(ref, h, p):
        return ref.at[p * rows : (p + 1) * rows, h]

    reads = [
        pltpu.make_async_copy(of(state_hbm, *c), old.at[c], in_sems.at[i])
        for i, c in enumerate(chunks)
    ]
    writes = [
        pltpu.make_async_copy(fresh.at[c], of(fresh_hbm, *c), out_sems.at[i])
        for i, c in enumerate(chunks)
    ]
    weights = [
        pltpu.make_async_copy(gate_hbm, gate_ref, in_sems.at[len(chunks)]),
        pltpu.make_async_copy(up_hbm, up_ref, in_sems.at[len(chunks) + 1]),
    ]
    for copy in reads + weights:
        copy.start()
    forget, key = turned(forget_ref[...], heads), turned(key_ref[...], heads)
    for i, (h, p) in enumerate(chunks):
        reads[i].wait()
        for r in range(rows):
            s = p * rows + r
            at = h * pieces * rows + s
            written = input_ref[s : s + 1, h * width : (h + 1) * width]
            fresh[h, p, r] = (
                forget[:, at : at + 1] * old[h, p, r] + key[:, at : at + 1] * written
            )
        writes[i].start()
    for copy in weights + writes:
        copy.wait()


def beside(forget, key, input_val, gate, up, state):
    seqs, heads, width, _ = state.shape
    pieces = 2 if seqs % 2 == 0 else 1
    buffer = pltpu.VMEM((heads, pieces, seqs // pieces, width, width), jnp.float32)
    return pl.pallas_call(
        beside_kernel,
        out_shape=(
            pltpu.VMEM(gate.shape, gate.dtype),
            pltpu.VMEM(up.shape, up.dtype),
            jax.ShapeDtypeStruct(state.shape, jnp.float32),
        ),
        in_specs=[VMEM] * 3 + [HBM] * 3,
        out_specs=(VMEM, VMEM, HBM),
        scratch_shapes=[
            buffer,
            buffer,
            pltpu.SemaphoreType.DMA((heads * pieces + 2,)),
            pltpu.SemaphoreType.DMA((heads * pieces,)),
        ],
        compiler_params=pltpu.CompilerParams(vmem_limit_bytes=12 << 20),
        name="beside",
    )(forget, key, input_val, *in_hbm(gate, up, state))


def expert_kernel(x_ref, gate_ref, up_ref, *refs):
    sources, out_ref, weights, sems = refs[:4], refs[4], refs[5:9], refs[9]
    copies = [pltpu.make_async_copy(sources[i], weights[i], sems.at[i]) for i in range(4)]
    for copy in copies:
        copy.start()
    x = x_ref[...]
    near = (silu(dot(x, gate_ref[...])) * dot(x, up_ref[...])).astype(jnp.bfloat16)
    copies[0].wait()
    gate = silu(dot(x, weights[0][...]))
    copies[1].wait()
    far = (gate * dot(x, weights[1][...])).astype(jnp.bfloat16)
    copies[2].wait()
    copies[3].wait()
    total = dot(near, weights[2][...]) + dot(far, weights[3][...])
    out_ref[...] = total.astype(jnp.bfloat16)


def expert(x, own, other):
    gate, up, down = own
    sources = (other[0], other[1], down, other[2])
    return pl.pallas_call(
        expert_kernel,
        out_shape=jax.ShapeDtypeStruct(x.shape, jnp.bfloat16),
        in_specs=[VMEM] * 3 + [HBM] * 4,
        out_specs=VMEM,
        scratch_shapes=[pltpu.VMEM(w.shape, w.dtype) for w in sources]
        + [pltpu.SemaphoreType.DMA((4,))],
        compiler_params=pltpu.CompilerParams(vmem_limit_bytes=10 << 20),
        name="expert",
    )(
        x,
        pltpu.with_memory_space_constraint(gate, pltpu.VMEM),
        pltpu.with_memory_space_constraint(up, pltpu.VMEM),
        *in_hbm(*sources),
    )


def shared_kernel(x_ref, *refs):
    sources, out_ref, weights, sems = refs[:3], refs[3], refs[4:7], refs[7]
    copies = [pltpu.make_async_copy(sources[i], weights[i], sems.at[i]) for i in range(3)]
    for copy in copies:
        copy.start()
    x = x_ref[...]
    copies[0].wait()
    gate = silu(dot(x, weights[0][...]))
    copies[1].wait()
    hidden = (gate * dot(x, weights[1][...])).astype(jnp.bfloat16)
    copies[2].wait()
    out_ref[...] = dot(hidden, weights[2][...]).astype(jnp.bfloat16)


def shared_expert(x, *weights):
    return pl.pallas_call(
        shared_kernel,
        out_shape=jax.ShapeDtypeStruct(x.shape, jnp.bfloat16),
        in_specs=[VMEM] + [HBM] * 3,
        out_specs=VMEM,
        scratch_shapes=[pltpu.VMEM(w.shape, w.dtype) for w in weights]
        + [pltpu.SemaphoreType.DMA((3,))],
        cost_estimate=pl.CostEstimate(
            flops=10_000_000_000, bytes_accessed=3 << 20, transcendentals=0
        ),
        compiler_params=pltpu.CompilerParams(vmem_limit_bytes=6 << 20),
        name="shared_expert",
    )(x, *in_hbm(*weights))


def combine_kernel(returned_ref, weight_ref, kept_ref, far_ref):
    blocks, rows, _ = returned_ref.shape
    total = 0.0
    for e in range(blocks):
        total = total + weight_ref[:, e : e + 1] * returned_ref[e].astype(jnp.float32)
    kept_ref[...] = total[: rows // 2]
    far_ref[...] = total[rows // 2 :].astype(jnp.bfloat16)


def combine(returned, weight):
    _, rows, width = returned.shape
    shape = (rows // 2, width)
    return pl.pallas_call(
        combine_kernel,
        out_shape=(
            jax.ShapeDtypeStruct(shape, jnp.float32),
            jax.ShapeDtypeStruct(shape, jnp.bfloat16),
        ),
        in_specs=[VMEM] * 2,
        out_specs=(VMEM,) * 2,
        compiler_params=pltpu.CompilerParams(vmem_limit_bytes=4 << 20),
        name="combine",
    )(returned, weight)


def part_of(which, size):
    return pl.ds(pl.multiple_of(which * size, size), size)


def divide_kernel(which_ref, kept_ref, far_ref, shared_ref, keeping_ref, giving_ref, both, wide):
    which, rows = which_ref[0], kept_ref.shape[0]
    wide[...] = shared_ref[...].astype(jnp.float32)
    both[:rows] = kept_ref[...] + far_ref[...].astype(jnp.float32) + wide[part_of(which, rows)]
    both[rows:] = wide[part_of(1 - which, rows)]
    width = keeping_ref.shape[1]
    keeping_ref[...] = both[:, part_of(which, width)]
    giving_ref[...] = both[:, part_of(1 - which, width)].astype(jnp.bfloat16)


def divide(which, kept, far, shared):
    rows, width = shared.shape
    shape = (rows, width // 2)
    return pl.pallas_call(
        divide_kernel,
        out_shape=(
            jax.ShapeDtypeStruct(shape, jnp.float32),
            jax.ShapeDtypeStruct(shape, jnp.bfloat16),
        ),
        in_specs=[pl.BlockSpec(memory_space=pltpu.SMEM)] + [VMEM] * 3,
        out_specs=(VMEM,) * 2,
        scratch_shapes=[pltpu.VMEM((rows, width), jnp.float32)] * 2,
        compiler_params=pltpu.CompilerParams(vmem_limit_bytes=4 << 20),
        name="divide",
    )(which, kept, far, shared)


def finish_kernel(which_ref, residual_ref, keeping_ref, got_ref, out_ref, total):
    which, rows = which_ref[0], out_ref.shape[0] // 2
    got = got_ref[...].astype(jnp.float32)
    total[part_of(which, rows)] = keeping_ref[:rows] + got[rows:]
    total[part_of(1 - which, rows)] = keeping_ref[rows:] + got[:rows]
    here = residual_ref[:, part_of(which, out_ref.shape[1])]
    out_ref[...] = (here + total[...]).astype(jnp.bfloat16)


def finish(which, residual, keeping, got):
    return pl.pallas_call(
        finish_kernel,
        out_shape=jax.ShapeDtypeStruct(got.shape, jnp.bfloat16),
        in_specs=[pl.BlockSpec(memory_space=pltpu.SMEM)] + [VMEM] * 3,
        out_specs=VMEM,
        scratch_shapes=[pltpu.VMEM(got.shape, jnp.float32)],
        compiler_params=pltpu.CompilerParams(vmem_limit_bytes=4 << 20),
        name="finish",
    )(which, residual, keeping, got)


def local(
    tokens,
    state,
    mix_gain,
    moe_gain,
    head_gain,
    w_forget,
    w_query,
    w_input,
    w_outgate,
    lower_bound,
    w_mix_out,
    routes,
    route_scores,
    expert_gate,
    expert_up,
    expert_down,
    shared_gate,
    shared_up,
    shared_down,
):
    seqs_here, full_width = tokens.shape
    n_ep = lax.axis_size("ep")
    n_tp = lax.axis_size("tp")
    tp_index = lax.axis_index("tp")
    half_rows = seqs_here // n_tp
    which_core = tp_index.reshape(1).astype(jnp.int32)

    mix_part, forget, key_gate, input_val = mixer(
        tokens,
        mix_gain,
        head_gain,
        lower_bound,
        w_forget,
        w_query,
        w_input,
        w_outgate,
        state,
        w_mix_out,
    )
    mixer_out = mix_part.astype(jnp.float32) + swap(mix_part).astype(jnp.float32)
    residual = tokens.astype(jnp.float32) + mixer_out.astype(jnp.bfloat16).astype(jnp.float32)
    moe_rows = rms_scale(residual, moe_gain).astype(jnp.bfloat16)

    half_ep = n_ep // 2
    halves = [list(range(half_ep)), list(range(half_ep, n_ep))]

    def across(values):
        return lax.ppermute(values, "ep", [(i, (i + half_ep) % n_ep) for i in range(n_ep)])

    own_rows = lax.dynamic_slice_in_dim(moe_rows, tp_index * half_rows, half_rows, 0)
    far_rows = across(own_rows)
    both_rows = jnp.concatenate([own_rows, far_rows], axis=0)
    outgoing = jnp.broadcast_to(both_rows[None], (half_ep, seqs_here, full_width))
    own = (expert_gate[0], expert_up[0], expert_down[0])
    *own_late, _ = lax.optimization_barrier((*own, own_rows))
    other = tuple(swap(w) for w in own_late)
    arrived = lax.all_to_all(outgoing, "ep", 0, 0, axis_index_groups=halves)
    arrived = arrived.reshape(half_ep * seqs_here, full_width)

    weights = route_scores / jnp.sum(route_scores, axis=-1, keepdims=True) * routed_scale
    chosen = routes[:, :, None] == jnp.arange(n_ep, dtype=jnp.int32)[None, None, :]
    expert_weight = jnp.sum(jnp.where(chosen, weights[:, :, None], 0.0), axis=1)
    expert_weight = lax.dynamic_slice_in_dim(expert_weight, tp_index * half_rows, half_rows, 0)
    expert_weight = expert_weight.reshape(half_rows, 2, half_ep)
    which = lax.axis_index("ep") // half_ep
    near = lax.dynamic_index_in_dim(expert_weight, which, 1, keepdims=False)
    far = lax.dynamic_index_in_dim(expert_weight, 1 - which, 1, keepdims=False)
    far = across(far)
    block_weight = jnp.concatenate([near, far], axis=0)

    shared_part = shared_expert(moe_rows, shared_gate, shared_up, shared_down)
    *ready, new_state = beside(forget, key_gate, input_val, own[0], own[1], state)
    leaving = expert(arrived, (*ready, own[2]), other).reshape(half_ep, seqs_here, full_width)
    returned = lax.all_to_all(leaving, "ep", 0, 0, axis_index_groups=halves)
    kept, far = combine(returned, block_weight)
    far = across(far)
    keeping, giving = divide(which_core, kept, far, shared_part)
    got = swap(giving)
    layer_out = finish(which_core, residual, keeping, got)
    return (layer_out, new_state)


def solution(mesh):
    return jax.shard_map(
        local,
        mesh=mesh,
        in_specs=(
            P("ep", None),
            P("ep", "tp", None, None),
            P(),
            P(),
            P(),
            P(None, "tp"),
            P(None, "tp"),
            P(None, "tp"),
            P(None, "tp"),
            P("tp"),
            P("tp", None),
            P("ep", None),
            P("ep", None),
            P("ep", None, "tp"),
            P("ep", None, "tp"),
            P("ep", "tp", None),
            P(None, "tp"),
            P(None, "tp"),
            P("tp", None),
        ),
        out_specs=(P("ep", "tp"), P("ep", "tp", None, None)),
        check_vma=False,
    )
```

```python
import jax
import jax.numpy as jnp
from jax import lax
from jax.experimental import pallas as pl
from jax.experimental.pallas import tpu as pltpu
from jax.sharding import PartitionSpec as P


epsilon = 1e-06
routed_scale = 2.5
HBM = pl.BlockSpec(memory_space=pltpu.HBM)
VMEM = pl.BlockSpec(memory_space=pltpu.VMEM)


def rms_scale(values, gain):
    return values * lax.rsqrt(jnp.mean(values * values, axis=-1, keepdims=True) + epsilon) * gain


def dot(a, b):
    return jnp.dot(a, b, preferred_element_type=jnp.float32)


def silu(values):
    return values / (1.0 + jnp.exp(-values))


def sigmoid(values):
    return 1.0 / (1.0 + jnp.exp(-values))


def swap(values):
    return lax.ppermute(values, "tp", [(0, 1), (1, 0)])


def in_hbm(*values):
    return tuple(pltpu.with_memory_space_constraint(v, pltpu.HBM) for v in values)


def turned(values, heads):
    rows, width = values.shape[0], values.shape[1] // heads
    parts = [values[:, h * width : (h + 1) * width] for h in range(heads)]
    if width > rows * heads:
        parts.append(jnp.zeros((width - rows * heads, width), jnp.float32))
    return jnp.concatenate(parts, axis=0).T


def mixer_kernel(*refs):
    sources, refs = refs[:10], refs[10:]
    part_ref, forget_ref, key_ref, input_ref = refs[:4]
    targets, readout_ref, sems = refs[4:14], refs[14], refs[15]
    tokens_ref, mix_gain, bound_ref, wf, wq, wi, wg, head_gain, state, wm = targets
    state_hbm, wm_hbm = sources[8], sources[9]
    heads, seqs, width, _ = state.shape
    half = wm.shape[0] // 2
    copies = {}

    def start(name, source, target):
        copies[name] = pltpu.make_async_copy(source, target, sems.at[len(copies)])
        copies[name].start()

    def start_state(h):
        start(h, state_hbm.at[:, h], state.at[h])

    def start_mix(name, at):
        start(name, wm_hbm.at[at : at + half], wm.at[at : at + half])

    for name, i in (("tokens", 0), ("gain", 1), ("bound", 2), ("head", 7), ("f", 3), ("q", 4)):
        start(name, sources[i], targets[i])
    for h in range(heads):
        start_state(h)
    start("i", sources[5], wi)
    start("g", sources[6], wg)
    start_mix("m0", 0)
    start_mix("m1", half)
    copies["tokens"].wait()
    copies["gain"].wait()
    tokens = tokens_ref[...].astype(jnp.float32)
    normed = rms_scale(tokens, mix_gain[...]).astype(jnp.bfloat16)
    copies["bound"].wait()
    bound = bound_ref[...]
    copies["f"].wait()
    forget_pre = dot(normed, wf[...])
    forget = bound + (1.0 - bound) * sigmoid(forget_pre)
    key = (1.0 - bound) * sigmoid(-forget_pre)
    forget_ref[...] = forget
    key_ref[...] = key
    copies["q"].wait()
    query = silu(dot(normed, wq[...]))
    key_query = key * query
    columns = turned(forget * query, heads)

    def read_out(h):
        copies[h].wait()
        for s in range(seqs):
            at = h * seqs + s
            readout_ref[h, s : s + 1, :] = jnp.sum(
                state[h, s] * columns[:, at : at + 1], axis=0, keepdims=True
            )

    for h in range(heads):
        read_out(h)
    copies["i"].wait()
    input_val = dot(normed, wi[...])
    input_ref[...] = input_val
    copies["g"].wait()
    gate = silu(dot(normed, wg[...]))
    copies["head"].wait()
    done = []
    for h in range(heads):
        here = slice(h * width, (h + 1) * width)
        fresh = jnp.sum(key_query[:, here], axis=-1, keepdims=True) * input_val[:, here]
        readout = readout_ref[h] + fresh
        done.append((rms_scale(readout, head_gain[...]) * gate[:, here]).astype(jnp.bfloat16))
    done = jnp.concatenate(done, axis=1)
    copies["m0"].wait()
    copies["m1"].wait()
    part_ref[...] = dot(done, wm[...]).astype(jnp.bfloat16)


def mixer(tokens, mix_gain, head_gain, bound, wf, wq, wi, wg, state, wm):
    seqs, heads, width, _ = state.shape
    wide = jax.ShapeDtypeStruct((seqs, heads * width), jnp.float32)
    sources = (tokens, mix_gain[None], bound[None], wf, wq, wi, wg, head_gain[None], state, wm)
    held = [pltpu.VMEM(w.shape, w.dtype) for w in sources]
    held[8] = pltpu.VMEM((heads, seqs, width, width), jnp.float32)
    return pl.pallas_call(
        mixer_kernel,
        out_shape=(jax.ShapeDtypeStruct((seqs, wm.shape[1]), jnp.bfloat16), wide, wide, wide),
        in_specs=[HBM] * len(sources),
        out_specs=(VMEM,) * 4,
        scratch_shapes=held
        + [
            pltpu.VMEM((heads, seqs, width), jnp.float32),
            pltpu.SemaphoreType.DMA((len(sources) + heads,)),
        ],
        cost_estimate=pl.CostEstimate(
            flops=40_000_000_000, bytes_accessed=16 << 20, transcendentals=0
        ),
        compiler_params=pltpu.CompilerParams(vmem_limit_bytes=20 << 20),
        name="mixer",
    )(*in_hbm(*sources))


def beside_kernel(forget_ref, key_ref, input_ref, gate_hbm, up_hbm, state_hbm, *refs):
    gate_ref, up_ref, fresh_hbm, old, fresh, in_sems, out_sems = refs
    heads, pieces, rows = old.shape[:3]
    width = old.shape[-1]
    chunks = [(h, p) for h in range(heads) for p in range(pieces)]

    def of(ref, h, p):
        return ref.at[p * rows : (p + 1) * rows, h]

    reads = [
        pltpu.make_async_copy(of(state_hbm, *c), old.at[c], in_sems.at[i])
        for i, c in enumerate(chunks)
    ]
    writes = [
        pltpu.make_async_copy(fresh.at[c], of(fresh_hbm, *c), out_sems.at[i])
        for i, c in enumerate(chunks)
    ]
    weights = [
        pltpu.make_async_copy(gate_hbm, gate_ref, in_sems.at[len(chunks)]),
        pltpu.make_async_copy(up_hbm, up_ref, in_sems.at[len(chunks) + 1]),
    ]
    for copy in reads + weights:
        copy.start()
    forget, key = turned(forget_ref[...], heads), turned(key_ref[...], heads)
    for i, (h, p) in enumerate(chunks):
        reads[i].wait()
        for r in range(rows):
            s = p * rows + r
            at = h * pieces * rows + s
            written = input_ref[s : s + 1, h * width : (h + 1) * width]
            fresh[h, p, r] = (
                forget[:, at : at + 1] * old[h, p, r] + key[:, at : at + 1] * written
            )
        writes[i].start()
    for copy in weights + writes:
        copy.wait()


def beside(forget, key, input_val, gate, up, state):
    seqs, heads, width, _ = state.shape
    pieces = 2 if seqs % 2 == 0 else 1
    buffer = pltpu.VMEM((heads, pieces, seqs // pieces, width, width), jnp.float32)
    return pl.pallas_call(
        beside_kernel,
        out_shape=(
            pltpu.VMEM(gate.shape, gate.dtype),
            pltpu.VMEM(up.shape, up.dtype),
            jax.ShapeDtypeStruct(state.shape, jnp.float32),
        ),
        in_specs=[VMEM] * 3 + [HBM] * 3,
        out_specs=(VMEM, VMEM, HBM),
        scratch_shapes=[
            buffer,
            buffer,
            pltpu.SemaphoreType.DMA((heads * pieces + 2,)),
            pltpu.SemaphoreType.DMA((heads * pieces,)),
        ],
        compiler_params=pltpu.CompilerParams(vmem_limit_bytes=12 << 20),
        name="beside",
    )(forget, key, input_val, *in_hbm(gate, up, state))


def expert_kernel(x_ref, gate_ref, up_ref, *refs):
    sources, out_ref, weights, sems = refs[:4], refs[4], refs[5:9], refs[9]
    copies = [pltpu.make_async_copy(sources[i], weights[i], sems.at[i]) for i in range(4)]
    for copy in copies:
        copy.start()
    x = x_ref[...]
    near = (silu(dot(x, gate_ref[...])) * dot(x, up_ref[...])).astype(jnp.bfloat16)
    copies[0].wait()
    gate = silu(dot(x, weights[0][...]))
    copies[1].wait()
    far = (gate * dot(x, weights[1][...])).astype(jnp.bfloat16)
    copies[2].wait()
    copies[3].wait()
    total = dot(near, weights[2][...]) + dot(far, weights[3][...])
    out_ref[...] = total.astype(jnp.bfloat16)


def expert(x, own, other):
    gate, up, down = own
    sources = (other[0], other[1], down, other[2])
    return pl.pallas_call(
        expert_kernel,
        out_shape=jax.ShapeDtypeStruct(x.shape, jnp.bfloat16),
        in_specs=[VMEM] * 3 + [HBM] * 4,
        out_specs=VMEM,
        scratch_shapes=[pltpu.VMEM(w.shape, w.dtype) for w in sources]
        + [pltpu.SemaphoreType.DMA((4,))],
        compiler_params=pltpu.CompilerParams(vmem_limit_bytes=10 << 20),
        name="expert",
    )(
        x,
        pltpu.with_memory_space_constraint(gate, pltpu.VMEM),
        pltpu.with_memory_space_constraint(up, pltpu.VMEM),
        *in_hbm(*sources),
    )


def shared_kernel(x_ref, *refs):
    sources, out_ref, weights, sems = refs[:3], refs[3], refs[4:7], refs[7]
    copies = [pltpu.make_async_copy(sources[i], weights[i], sems.at[i]) for i in range(3)]
    for copy in copies:
        copy.start()
    x = x_ref[...]
    copies[0].wait()
    gate = silu(dot(x, weights[0][...]))
    copies[1].wait()
    hidden = (gate * dot(x, weights[1][...])).astype(jnp.bfloat16)
    copies[2].wait()
    out_ref[...] = dot(hidden, weights[2][...]).astype(jnp.bfloat16)


def shared_expert(x, *weights):
    return pl.pallas_call(
        shared_kernel,
        out_shape=jax.ShapeDtypeStruct(x.shape, jnp.bfloat16),
        in_specs=[VMEM] + [HBM] * 3,
        out_specs=VMEM,
        scratch_shapes=[pltpu.VMEM(w.shape, w.dtype) for w in weights]
        + [pltpu.SemaphoreType.DMA((3,))],
        cost_estimate=pl.CostEstimate(
            flops=10_000_000_000, bytes_accessed=3 << 20, transcendentals=0
        ),
        compiler_params=pltpu.CompilerParams(vmem_limit_bytes=6 << 20),
        name="shared_expert",
    )(x, *in_hbm(*weights))


def combine_kernel(returned_ref, weight_ref, kept_ref, far_ref):
    blocks, rows, _ = returned_ref.shape
    total = 0.0
    for e in range(blocks):
        total = total + weight_ref[:, e : e + 1] * returned_ref[e].astype(jnp.float32)
    kept_ref[...] = total[: rows // 2]
    far_ref[...] = total[rows // 2 :].astype(jnp.bfloat16)


def combine(returned, weight):
    _, rows, width = returned.shape
    shape = (rows // 2, width)
    return pl.pallas_call(
        combine_kernel,
        out_shape=(
            jax.ShapeDtypeStruct(shape, jnp.float32),
            jax.ShapeDtypeStruct(shape, jnp.bfloat16),
        ),
        in_specs=[VMEM] * 2,
        out_specs=(VMEM,) * 2,
        compiler_params=pltpu.CompilerParams(vmem_limit_bytes=4 << 20),
        name="combine",
    )(returned, weight)


def part_of(which, size):
    return pl.ds(pl.multiple_of(which * size, size), size)


def divide_kernel(which_ref, kept_ref, far_ref, shared_ref, keeping_ref, giving_ref, both, wide):
    which, rows = which_ref[0], kept_ref.shape[0]
    wide[...] = shared_ref[...].astype(jnp.float32)
    both[:rows] = kept_ref[...] + far_ref[...].astype(jnp.float32) + wide[part_of(which, rows)]
    both[rows:] = wide[part_of(1 - which, rows)]
    width = keeping_ref.shape[1]
    keeping_ref[...] = both[:, part_of(which, width)]
    giving_ref[...] = both[:, part_of(1 - which, width)].astype(jnp.bfloat16)


def divide(which, kept, far, shared):
    rows, width = shared.shape
    shape = (rows, width // 2)
    return pl.pallas_call(
        divide_kernel,
        out_shape=(
            jax.ShapeDtypeStruct(shape, jnp.float32),
            jax.ShapeDtypeStruct(shape, jnp.bfloat16),
        ),
        in_specs=[pl.BlockSpec(memory_space=pltpu.SMEM)] + [VMEM] * 3,
        out_specs=(VMEM,) * 2,
        scratch_shapes=[pltpu.VMEM((rows, width), jnp.float32)] * 2,
        compiler_params=pltpu.CompilerParams(vmem_limit_bytes=4 << 20),
        name="divide",
    )(which, kept, far, shared)


def finish_kernel(which_ref, residual_ref, keeping_ref, got_ref, out_ref, total):
    which, rows = which_ref[0], out_ref.shape[0] // 2
    got = got_ref[...].astype(jnp.float32)
    total[part_of(which, rows)] = keeping_ref[:rows] + got[rows:]
    total[part_of(1 - which, rows)] = keeping_ref[rows:] + got[:rows]
    here = residual_ref[:, part_of(which, out_ref.shape[1])]
    out_ref[...] = (here + total[...]).astype(jnp.bfloat16)


def finish(which, residual, keeping, got):
    return pl.pallas_call(
        finish_kernel,
        out_shape=jax.ShapeDtypeStruct(got.shape, jnp.bfloat16),
        in_specs=[pl.BlockSpec(memory_space=pltpu.SMEM)] + [VMEM] * 3,
        out_specs=VMEM,
        scratch_shapes=[pltpu.VMEM(got.shape, jnp.float32)],
        compiler_params=pltpu.CompilerParams(vmem_limit_bytes=4 << 20),
        name="finish",
    )(which, residual, keeping, got)


def route_kernel(which_ref, tokens_ref, part_ref, other_ref, gain_ref, *refs):
    residual_ref, rows_ref, own_ref, normed = refs
    mixed = part_ref[...].astype(jnp.float32) + other_ref[...].astype(jnp.float32)
    mixed = mixed.astype(jnp.bfloat16).astype(jnp.float32)
    residual = tokens_ref[...].astype(jnp.float32) + mixed
    residual_ref[...] = residual
    normed[...] = rms_scale(residual, gain_ref[...])
    rows_ref[...] = normed[...].astype(jnp.bfloat16)
    own_ref[...] = normed[part_of(which_ref[0], own_ref.shape[0])].astype(jnp.bfloat16)


def route(which, tokens, part, other, gain, own_rows):
    shape = tokens.shape
    return pl.pallas_call(
        route_kernel,
        out_shape=(
            jax.ShapeDtypeStruct(shape, jnp.float32),
            jax.ShapeDtypeStruct(shape, jnp.bfloat16),
            jax.ShapeDtypeStruct((own_rows, shape[1]), jnp.bfloat16),
        ),
        in_specs=[pl.BlockSpec(memory_space=pltpu.SMEM)] + [VMEM] * 4,
        out_specs=(VMEM,) * 3,
        scratch_shapes=[pltpu.VMEM(shape, jnp.float32)],
        compiler_params=pltpu.CompilerParams(vmem_limit_bytes=4 << 20),
        name="route",
    )(which, tokens, part, other, gain[None])


def local(
    tokens,
    state,
    mix_gain,
    moe_gain,
    head_gain,
    w_forget,
    w_query,
    w_input,
    w_outgate,
    lower_bound,
    w_mix_out,
    routes,
    route_scores,
    expert_gate,
    expert_up,
    expert_down,
    shared_gate,
    shared_up,
    shared_down,
):
    seqs_here, full_width = tokens.shape
    n_ep = lax.axis_size("ep")
    n_tp = lax.axis_size("tp")
    tp_index = lax.axis_index("tp")
    half_rows = seqs_here // n_tp
    which_core = tp_index.reshape(1).astype(jnp.int32)

    mix_part, forget, key_gate, input_val = mixer(
        tokens,
        mix_gain,
        head_gain,
        lower_bound,
        w_forget,
        w_query,
        w_input,
        w_outgate,
        state,
        w_mix_out,
    )
    residual, moe_rows, own_rows = route(
        which_core, tokens, mix_part, swap(mix_part), moe_gain, half_rows
    )

    half_ep = n_ep // 2
    halves = [list(range(half_ep)), list(range(half_ep, n_ep))]

    def across(values):
        return lax.ppermute(values, "ep", [(i, (i + half_ep) % n_ep) for i in range(n_ep)])

    far_rows = across(own_rows)
    both_rows = jnp.concatenate([own_rows, far_rows], axis=0)
    outgoing = jnp.broadcast_to(both_rows[None], (half_ep, seqs_here, full_width))
    own = (expert_gate[0], expert_up[0], expert_down[0])
    *own_late, _ = lax.optimization_barrier((*own, own_rows))
    other = tuple(swap(w) for w in own_late)
    arrived = lax.all_to_all(outgoing, "ep", 0, 0, axis_index_groups=halves)
    arrived = arrived.reshape(half_ep * seqs_here, full_width)

    weights = route_scores / jnp.sum(route_scores, axis=-1, keepdims=True) * routed_scale
    chosen = routes[:, :, None] == jnp.arange(n_ep, dtype=jnp.int32)[None, None, :]
    expert_weight = jnp.sum(jnp.where(chosen, weights[:, :, None], 0.0), axis=1)
    expert_weight = lax.dynamic_slice_in_dim(expert_weight, tp_index * half_rows, half_rows, 0)
    expert_weight = expert_weight.reshape(half_rows, 2, half_ep)
    which = lax.axis_index("ep") // half_ep
    near = lax.dynamic_index_in_dim(expert_weight, which, 1, keepdims=False)
    far = lax.dynamic_index_in_dim(expert_weight, 1 - which, 1, keepdims=False)
    far = across(far)
    block_weight = jnp.concatenate([near, far], axis=0)

    shared_part = shared_expert(moe_rows, shared_gate, shared_up, shared_down)
    *ready, new_state = beside(forget, key_gate, input_val, own[0], own[1], state)
    leaving = expert(arrived, (*ready, own[2]), other).reshape(half_ep, seqs_here, full_width)
    returned = lax.all_to_all(leaving, "ep", 0, 0, axis_index_groups=halves)
    kept, far = combine(returned, block_weight)
    far = across(far)
    keeping, giving = divide(which_core, kept, far, shared_part)
    got = swap(giving)
    layer_out = finish(which_core, residual, keeping, got)
    return (layer_out, new_state)


def solution(mesh):
    return jax.shard_map(
        local,
        mesh=mesh,
        in_specs=(
            P("ep", None),
            P("ep", "tp", None, None),
            P(),
            P(),
            P(),
            P(None, "tp"),
            P(None, "tp"),
            P(None, "tp"),
            P(None, "tp"),
            P("tp"),
            P("tp", None),
            P("ep", None),
            P("ep", None),
            P("ep", None, "tp"),
            P("ep", None, "tp"),
            P("ep", "tp", None),
            P(None, "tp"),
            P(None, "tp"),
            P("tp", None),
        ),
        out_specs=(P("ep", "tp"), P("ep", "tp", None, None)),
        check_vma=False,
    )
```

```python
import jax
import jax.numpy as jnp
from jax import lax
from jax.experimental import pallas as pl
from jax.experimental.pallas import tpu as pltpu
from jax.sharding import PartitionSpec as P


epsilon = 1e-06
routed_scale = 2.5
HBM = pl.BlockSpec(memory_space=pltpu.HBM)
VMEM = pl.BlockSpec(memory_space=pltpu.VMEM)


def rms_scale(values, gain):
    return values * lax.rsqrt(jnp.mean(values * values, axis=-1, keepdims=True) + epsilon) * gain


def dot(a, b):
    return jnp.dot(a, b, preferred_element_type=jnp.float32)


def silu(values):
    return values / (1.0 + jnp.exp(-values))


def sigmoid(values):
    return 1.0 / (1.0 + jnp.exp(-values))


def swap(values):
    return lax.ppermute(values, "tp", [(0, 1), (1, 0)])


def in_hbm(*values):
    return tuple(pltpu.with_memory_space_constraint(v, pltpu.HBM) for v in values)


def turned(values, heads):
    rows, width = values.shape[0], values.shape[1] // heads
    parts = [values[:, h * width : (h + 1) * width] for h in range(heads)]
    if width > rows * heads:
        parts.append(jnp.zeros((width - rows * heads, width), jnp.float32))
    return jnp.concatenate(parts, axis=0).T


def mixer_kernel(*refs):
    sources, refs = refs[:10], refs[10:]
    part_ref, forget_ref, key_ref, input_ref = refs[:4]
    targets, readout_ref, sems = refs[4:14], refs[14], refs[15]
    tokens_ref, mix_gain, bound_ref, wf, wq, wi, wg, head_gain, state, wm = targets
    state_hbm, wm_hbm = sources[8], sources[9]
    heads, seqs, width, _ = state.shape
    half = wm.shape[0] // 2
    copies = {}

    def start(name, source, target):
        copies[name] = pltpu.make_async_copy(source, target, sems.at[len(copies)])
        copies[name].start()

    def start_state(h):
        start(h, state_hbm.at[:, h], state.at[h])

    def start_mix(name, at):
        start(name, wm_hbm.at[at : at + half], wm.at[at : at + half])

    for name, i in (("tokens", 0), ("gain", 1), ("bound", 2), ("head", 7), ("f", 3), ("q", 4)):
        start(name, sources[i], targets[i])
    for h in range(heads):
        start_state(h)
    start("i", sources[5], wi)
    start("g", sources[6], wg)
    start_mix("m0", 0)
    start_mix("m1", half)
    copies["tokens"].wait()
    copies["gain"].wait()
    tokens = tokens_ref[...].astype(jnp.float32)
    normed = rms_scale(tokens, mix_gain[...]).astype(jnp.bfloat16)
    copies["bound"].wait()
    bound = bound_ref[...]
    copies["f"].wait()
    forget_pre = dot(normed, wf[...])
    forget = bound + (1.0 - bound) * sigmoid(forget_pre)
    key = (1.0 - bound) * sigmoid(-forget_pre)
    forget_ref[...] = forget
    key_ref[...] = key
    copies["q"].wait()
    query = silu(dot(normed, wq[...]))
    key_query = key * query
    columns = turned(forget * query, heads)

    def read_out(h):
        copies[h].wait()
        for s in range(seqs):
            at = h * seqs + s
            readout_ref[h, s : s + 1, :] = jnp.sum(
                state[h, s] * columns[:, at : at + 1], axis=0, keepdims=True
            )

    for h in range(heads):
        read_out(h)
    copies["i"].wait()
    input_val = dot(normed, wi[...])
    input_ref[...] = input_val
    copies["g"].wait()
    gate = silu(dot(normed, wg[...]))
    copies["head"].wait()
    done = []
    for h in range(heads):
        here = slice(h * width, (h + 1) * width)
        fresh = jnp.sum(key_query[:, here], axis=-1, keepdims=True) * input_val[:, here]
        readout = readout_ref[h] + fresh
        done.append((rms_scale(readout, head_gain[...]) * gate[:, here]).astype(jnp.bfloat16))
    done = jnp.concatenate(done, axis=1)
    copies["m0"].wait()
    copies["m1"].wait()
    part_ref[...] = dot(done, wm[...]).astype(jnp.bfloat16)


def mixer(tokens, mix_gain, head_gain, bound, wf, wq, wi, wg, state, wm):
    seqs, heads, width, _ = state.shape
    wide = jax.ShapeDtypeStruct((seqs, heads * width), jnp.float32)
    sources = (tokens, mix_gain[None], bound[None], wf, wq, wi, wg, head_gain[None], state, wm)
    held = [pltpu.VMEM(w.shape, w.dtype) for w in sources]
    held[8] = pltpu.VMEM((heads, seqs, width, width), jnp.float32)
    return pl.pallas_call(
        mixer_kernel,
        out_shape=(jax.ShapeDtypeStruct((seqs, wm.shape[1]), jnp.bfloat16), wide, wide, wide),
        in_specs=[HBM] * len(sources),
        out_specs=(VMEM,) * 4,
        scratch_shapes=held
        + [
            pltpu.VMEM((heads, seqs, width), jnp.float32),
            pltpu.SemaphoreType.DMA((len(sources) + heads,)),
        ],
        cost_estimate=pl.CostEstimate(
            flops=40_000_000_000, bytes_accessed=16 << 20, transcendentals=0
        ),
        compiler_params=pltpu.CompilerParams(vmem_limit_bytes=20 << 20),
        name="mixer",
    )(*in_hbm(*sources))


def beside_kernel(forget_ref, key_ref, input_ref, gate_hbm, up_hbm, state_hbm, *refs):
    gate_ref, up_ref, fresh_hbm, old, fresh, in_sems, out_sems = refs
    heads, pieces, rows = old.shape[:3]
    width = old.shape[-1]
    chunks = [(h, p) for h in range(heads) for p in range(pieces)]

    def of(ref, h, p):
        return ref.at[p * rows : (p + 1) * rows, h]

    reads = [
        pltpu.make_async_copy(of(state_hbm, *c), old.at[c], in_sems.at[i])
        for i, c in enumerate(chunks)
    ]
    writes = [
        pltpu.make_async_copy(fresh.at[c], of(fresh_hbm, *c), out_sems.at[i])
        for i, c in enumerate(chunks)
    ]
    weights = [
        pltpu.make_async_copy(gate_hbm, gate_ref, in_sems.at[len(chunks)]),
        pltpu.make_async_copy(up_hbm, up_ref, in_sems.at[len(chunks) + 1]),
    ]
    for copy in reads + weights:
        copy.start()
    forget, key = turned(forget_ref[...], heads), turned(key_ref[...], heads)
    for i, (h, p) in enumerate(chunks):
        reads[i].wait()
        for r in range(rows):
            s = p * rows + r
            at = h * pieces * rows + s
            written = input_ref[s : s + 1, h * width : (h + 1) * width]
            fresh[h, p, r] = (
                forget[:, at : at + 1] * old[h, p, r] + key[:, at : at + 1] * written
            )
        writes[i].start()
    for copy in weights + writes:
        copy.wait()


def beside(forget, key, input_val, gate, up, state):
    seqs, heads, width, _ = state.shape
    pieces = 2 if seqs % 2 == 0 else 1
    buffer = pltpu.VMEM((heads, pieces, seqs // pieces, width, width), jnp.float32)
    return pl.pallas_call(
        beside_kernel,
        out_shape=(
            pltpu.VMEM(gate.shape, gate.dtype),
            pltpu.VMEM(up.shape, up.dtype),
            jax.ShapeDtypeStruct(state.shape, jnp.float32),
        ),
        in_specs=[VMEM] * 3 + [HBM] * 3,
        out_specs=(VMEM, VMEM, HBM),
        scratch_shapes=[
            buffer,
            buffer,
            pltpu.SemaphoreType.DMA((heads * pieces + 2,)),
            pltpu.SemaphoreType.DMA((heads * pieces,)),
        ],
        compiler_params=pltpu.CompilerParams(vmem_limit_bytes=12 << 20),
        name="beside",
    )(forget, key, input_val, *in_hbm(gate, up, state))


def expert_kernel(x_ref, gate_ref, up_ref, *refs):
    sources, out_ref, gate_far, up_far, down, sems = refs[:4], refs[4], *refs[5:8], refs[8]
    depth = sources[2].shape[0]
    targets = (gate_far, up_far, down.at[:depth], down.at[depth:])
    copies = [pltpu.make_async_copy(sources[i], targets[i], sems.at[i]) for i in range(4)]
    for copy in copies:
        copy.start()
    x = x_ref[...]
    near = (silu(dot(x, gate_ref[...])) * dot(x, up_ref[...])).astype(jnp.bfloat16)
    copies[0].wait()
    gate = silu(dot(x, gate_far[...]))
    copies[1].wait()
    far = (gate * dot(x, up_far[...])).astype(jnp.bfloat16)
    hidden = jnp.concatenate([near, far], axis=1)
    copies[2].wait()
    copies[3].wait()
    out_ref[...] = dot(hidden, down[...]).astype(jnp.bfloat16)


def expert(x, own, other):
    gate, up, down = own
    sources = (other[0], other[1], down, other[2])
    depth, width = down.shape
    return pl.pallas_call(
        expert_kernel,
        out_shape=jax.ShapeDtypeStruct(x.shape, jnp.bfloat16),
        in_specs=[VMEM] * 3 + [HBM] * 4,
        out_specs=VMEM,
        scratch_shapes=[
            pltpu.VMEM(gate.shape, gate.dtype),
            pltpu.VMEM(up.shape, up.dtype),
            pltpu.VMEM((2 * depth, width), down.dtype),
            pltpu.SemaphoreType.DMA((4,)),
        ],
        compiler_params=pltpu.CompilerParams(vmem_limit_bytes=10 << 20),
        name="expert",
    )(
        x,
        pltpu.with_memory_space_constraint(gate, pltpu.VMEM),
        pltpu.with_memory_space_constraint(up, pltpu.VMEM),
        *in_hbm(*sources),
    )


def shared_kernel(x_ref, *refs):
    sources, out_ref, weights, sems = refs[:3], refs[3], refs[4:7], refs[7]
    copies = [pltpu.make_async_copy(sources[i], weights[i], sems.at[i]) for i in range(3)]
    for copy in copies:
        copy.start()
    x = x_ref[...]
    copies[0].wait()
    gate = silu(dot(x, weights[0][...]))
    copies[1].wait()
    hidden = (gate * dot(x, weights[1][...])).astype(jnp.bfloat16)
    copies[2].wait()
    out_ref[...] = dot(hidden, weights[2][...]).astype(jnp.bfloat16)


def shared_expert(x, *weights):
    return pl.pallas_call(
        shared_kernel,
        out_shape=jax.ShapeDtypeStruct(x.shape, jnp.bfloat16),
        in_specs=[VMEM] + [HBM] * 3,
        out_specs=VMEM,
        scratch_shapes=[pltpu.VMEM(w.shape, w.dtype) for w in weights]
        + [pltpu.SemaphoreType.DMA((3,))],
        cost_estimate=pl.CostEstimate(
            flops=10_000_000_000, bytes_accessed=3 << 20, transcendentals=0
        ),
        compiler_params=pltpu.CompilerParams(vmem_limit_bytes=6 << 20),
        name="shared_expert",
    )(x, *in_hbm(*weights))


def combine_kernel(returned_ref, weight_ref, kept_ref, far_ref):
    blocks, rows, _ = returned_ref.shape
    total = 0.0
    for e in range(blocks):
        total = total + weight_ref[:, e : e + 1] * returned_ref[e].astype(jnp.float32)
    kept_ref[...] = total[: rows // 2]
    far_ref[...] = total[rows // 2 :].astype(jnp.bfloat16)


def combine(returned, weight):
    _, rows, width = returned.shape
    shape = (rows // 2, width)
    return pl.pallas_call(
        combine_kernel,
        out_shape=(
            jax.ShapeDtypeStruct(shape, jnp.float32),
            jax.ShapeDtypeStruct(shape, jnp.bfloat16),
        ),
        in_specs=[VMEM] * 2,
        out_specs=(VMEM,) * 2,
        compiler_params=pltpu.CompilerParams(vmem_limit_bytes=4 << 20),
        name="combine",
    )(returned, weight)


def part_of(which, size):
    return pl.ds(pl.multiple_of(which * size, size), size)


def divide_kernel(which_ref, kept_ref, far_ref, shared_ref, keeping_ref, giving_ref, both, wide):
    which, rows = which_ref[0], kept_ref.shape[0]
    wide[...] = shared_ref[...].astype(jnp.float32)
    both[:rows] = kept_ref[...] + far_ref[...].astype(jnp.float32) + wide[part_of(which, rows)]
    both[rows:] = wide[part_of(1 - which, rows)]
    width = keeping_ref.shape[1]
    keeping_ref[...] = both[:, part_of(which, width)]
    giving_ref[...] = both[:, part_of(1 - which, width)].astype(jnp.bfloat16)


def divide(which, kept, far, shared):
    rows, width = shared.shape
    shape = (rows, width // 2)
    return pl.pallas_call(
        divide_kernel,
        out_shape=(
            jax.ShapeDtypeStruct(shape, jnp.float32),
            jax.ShapeDtypeStruct(shape, jnp.bfloat16),
        ),
        in_specs=[pl.BlockSpec(memory_space=pltpu.SMEM)] + [VMEM] * 3,
        out_specs=(VMEM,) * 2,
        scratch_shapes=[pltpu.VMEM((rows, width), jnp.float32)] * 2,
        compiler_params=pltpu.CompilerParams(vmem_limit_bytes=4 << 20),
        name="divide",
    )(which, kept, far, shared)


def finish_kernel(which_ref, residual_ref, keeping_ref, got_ref, out_ref, total):
    which, rows = which_ref[0], out_ref.shape[0] // 2
    got = got_ref[...].astype(jnp.float32)
    total[part_of(which, rows)] = keeping_ref[:rows] + got[rows:]
    total[part_of(1 - which, rows)] = keeping_ref[rows:] + got[:rows]
    here = residual_ref[:, part_of(which, out_ref.shape[1])]
    out_ref[...] = (here + total[...]).astype(jnp.bfloat16)


def finish(which, residual, keeping, got):
    return pl.pallas_call(
        finish_kernel,
        out_shape=jax.ShapeDtypeStruct(got.shape, jnp.bfloat16),
        in_specs=[pl.BlockSpec(memory_space=pltpu.SMEM)] + [VMEM] * 3,
        out_specs=VMEM,
        scratch_shapes=[pltpu.VMEM(got.shape, jnp.float32)],
        compiler_params=pltpu.CompilerParams(vmem_limit_bytes=4 << 20),
        name="finish",
    )(which, residual, keeping, got)


def route_kernel(which_ref, tokens_ref, part_ref, other_ref, gain_ref, *refs):
    residual_ref, rows_ref, own_ref, normed = refs
    mixed = part_ref[...].astype(jnp.float32) + other_ref[...].astype(jnp.float32)
    mixed = mixed.astype(jnp.bfloat16).astype(jnp.float32)
    residual = tokens_ref[...].astype(jnp.float32) + mixed
    residual_ref[...] = residual
    normed[...] = rms_scale(residual, gain_ref[...])
    rows_ref[...] = normed[...].astype(jnp.bfloat16)
    own_ref[...] = normed[part_of(which_ref[0], own_ref.shape[0])].astype(jnp.bfloat16)


def route(which, tokens, part, other, gain, own_rows):
    shape = tokens.shape
    return pl.pallas_call(
        route_kernel,
        out_shape=(
            jax.ShapeDtypeStruct(shape, jnp.float32),
            jax.ShapeDtypeStruct(shape, jnp.bfloat16),
            jax.ShapeDtypeStruct((own_rows, shape[1]), jnp.bfloat16),
        ),
        in_specs=[pl.BlockSpec(memory_space=pltpu.SMEM)] + [VMEM] * 4,
        out_specs=(VMEM,) * 3,
        scratch_shapes=[pltpu.VMEM(shape, jnp.float32)],
        compiler_params=pltpu.CompilerParams(vmem_limit_bytes=4 << 20),
        name="route",
    )(which, tokens, part, other, gain[None])


def local(
    tokens,
    state,
    mix_gain,
    moe_gain,
    head_gain,
    w_forget,
    w_query,
    w_input,
    w_outgate,
    lower_bound,
    w_mix_out,
    routes,
    route_scores,
    expert_gate,
    expert_up,
    expert_down,
    shared_gate,
    shared_up,
    shared_down,
):
    seqs_here, full_width = tokens.shape
    n_ep = lax.axis_size("ep")
    n_tp = lax.axis_size("tp")
    tp_index = lax.axis_index("tp")
    half_rows = seqs_here // n_tp
    which_core = tp_index.reshape(1).astype(jnp.int32)

    mix_part, forget, key_gate, input_val = mixer(
        tokens,
        mix_gain,
        head_gain,
        lower_bound,
        w_forget,
        w_query,
        w_input,
        w_outgate,
        state,
        w_mix_out,
    )
    residual, moe_rows, own_rows = route(
        which_core, tokens, mix_part, swap(mix_part), moe_gain, half_rows
    )

    half_ep = n_ep // 2
    halves = [list(range(half_ep)), list(range(half_ep, n_ep))]

    def across(values):
        return lax.ppermute(values, "ep", [(i, (i + half_ep) % n_ep) for i in range(n_ep)])

    far_rows = across(own_rows)
    both_rows = jnp.concatenate([own_rows, far_rows], axis=0)
    outgoing = jnp.broadcast_to(both_rows[None], (half_ep, seqs_here, full_width))
    own = (expert_gate[0], expert_up[0], expert_down[0])
    *own_late, _ = lax.optimization_barrier((*own, own_rows))
    other = tuple(swap(w) for w in own_late)
    arrived = lax.all_to_all(outgoing, "ep", 0, 0, axis_index_groups=halves)
    arrived = arrived.reshape(half_ep * seqs_here, full_width)

    weights = route_scores / jnp.sum(route_scores, axis=-1, keepdims=True) * routed_scale
    chosen = routes[:, :, None] == jnp.arange(n_ep, dtype=jnp.int32)[None, None, :]
    expert_weight = jnp.sum(jnp.where(chosen, weights[:, :, None], 0.0), axis=1)
    expert_weight = lax.dynamic_slice_in_dim(expert_weight, tp_index * half_rows, half_rows, 0)
    expert_weight = expert_weight.reshape(half_rows, 2, half_ep)
    which = lax.axis_index("ep") // half_ep
    near = lax.dynamic_index_in_dim(expert_weight, which, 1, keepdims=False)
    far = lax.dynamic_index_in_dim(expert_weight, 1 - which, 1, keepdims=False)
    far = across(far)
    block_weight = jnp.concatenate([near, far], axis=0)

    shared_part = shared_expert(moe_rows, shared_gate, shared_up, shared_down)
    *ready, new_state = beside(forget, key_gate, input_val, own[0], own[1], state)
    leaving = expert(arrived, (*ready, own[2]), other).reshape(half_ep, seqs_here, full_width)
    returned = lax.all_to_all(leaving, "ep", 0, 0, axis_index_groups=halves)
    kept, far = combine(returned, block_weight)
    far = across(far)
    keeping, giving = divide(which_core, kept, far, shared_part)
    got = swap(giving)
    layer_out = finish(which_core, residual, keeping, got)
    return (layer_out, new_state)


def solution(mesh):
    return jax.shard_map(
        local,
        mesh=mesh,
        in_specs=(
            P("ep", None),
            P("ep", "tp", None, None),
            P(),
            P(),
            P(),
            P(None, "tp"),
            P(None, "tp"),
            P(None, "tp"),
            P(None, "tp"),
            P("tp"),
            P("tp", None),
            P("ep", None),
            P("ep", None),
            P("ep", None, "tp"),
            P("ep", None, "tp"),
            P("ep", "tp", None),
            P(None, "tp"),
            P(None, "tp"),
            P("tp", None),
        ),
        out_specs=(P("ep", "tp"), P("ep", "tp", None, None)),
        check_vma=False,
    )
```
